32 devices in a mesh: sp: 8 (over z, y), tp: 4 (over x, core).
Axes of the slice: x: 2, y: 2, z: 4, core: 2. Of those that a mesh axis runs over, the one named last changes fastest.
Arguments:
- queries: bfloat16 [4096, 512], P('sp', 'tp'), may hold values from -6 to 6
- keys: bfloat16 [4096, 512], P('sp', 'tp'), may hold values from -6 to 6
- values: bfloat16 [4096, 1024], P('sp', 'tp'), may hold values from -6 to 6
- input_gate_log: float32 [8, 4096], P('tp', 'sp'), may hold values from -5 to 128
- forget_gate_logits: float32 [8, 4096], P('tp', 'sp'), may hold values from 1 to 16
- extra_decay_log: float32 [8, 4096], P('tp', 'sp'), may hold values from -1 to 0
- output_gate_logits: bfloat16 [4096, 1024], P('sp', 'tp'), may hold values from -6 to 6
- head_norm_scale: float32 [1024], P('tp'), may hold values from 0.1 to 1.9
- layer_residual_input: bfloat16 [4096, 2048], P(('sp', 'tp')), may hold values from -6 to 6
- output_projection_weight: bfloat16 [1024, 2048], replicated, may hold values from -0.1875 to 0.1875
- expert_norm_scale: float32 [2048], replicated, may hold values from 0.1 to 1.9
- routing_expert_index: int32 [4096, 2], P(('sp', 'tp')), may hold values from 0 to 31, all different within a row; in each aligned block of 128 rows (0 to 127, 128 to 255, ...) at most 16 rows name the same one
- routing_expert_weight: float32 [4096, 2], P(('sp', 'tp')), may hold values from 0.2 to 1
- expert_gate_weight: bfloat16 [32, 2048, 1024], P(('sp', 'tp')), may hold values from -0.125 to 0.125
- expert_up_weight: bfloat16 [32, 2048, 1024], P(('sp', 'tp')), may hold values from -0.125 to 0.125
- expert_down_weight: bfloat16 [32, 1024, 2048], P(('sp', 'tp')), may hold values from -0.1875 to 0.1875
Outputs:
- result: bfloat16 [4096, 2048], P(('sp', 'tp'))
The draws below stay inside these ranges and needn't reach their ends.
Inputs may be any that keep to these rules, and one draw needn't show every extreme that they name: `routing_expert_index`: each row names 2 different experts. Within each aligned block of 128 rows (the rows of one device) no expert is named more than 16 times, a bound that some block reaches in every draw.
All inputs are finite; a program needn't handle non-finite values.
Results may differ from the reference program's by a relative error of at most 0.013.
Values may be sent and summed in bfloat16 or wider, within the bound.
A program may use at most 64 MiB of HBM per device.

```python
import math
import jax
import jax.numpy as jnp
import numpy as np
from jax import lax

D = 2048
HEADS = 8
DQK = 64
DV = 128
FF = 1024
TOP = 2
BLOCK = 128
TOK_DEV = 512
TOKENS = 4096
ROWS = 128
EXPERTS = 32
CAP = 16
N_SP = 8
N_TP = 4


def draw_input_gate_log(key, part):
    gate_values = jax.random.truncated_normal(jax.random.fold_in(key, 21), -5.0, 5.0, (HEADS, TOKENS), jnp.float32)
    return gate_values


def draw_forget_gate_logits(key, part):
    order_key, fast_key, jitter_key, shift_key = jax.random.split(jax.random.fold_in(key, 31), 4)
    head_order = jax.random.permutation(order_key, HEADS)
    slow_count = HEADS // 2
    is_slow = (head_order < slow_count)[:, None]
    fast_level = jax.random.uniform(fast_key, (HEADS, 1), jnp.float32, 3.5, 4.5)
    slow_level = jnp.log(jnp.float32(TOKENS)) + 1.5
    jitter = 0.7 * jax.random.truncated_normal(jitter_key, -2.0, 2.0, (HEADS, TOKENS), jnp.float32)
    device_shift = jax.random.uniform(shift_key, (HEADS, TOKENS // TOK_DEV, 1), jnp.float32, -0.35, 0.35)
    device_shift = jnp.broadcast_to(device_shift, (HEADS, TOKENS // TOK_DEV, TOK_DEV)).reshape(HEADS, TOKENS)
    return jnp.where(is_slow, slow_level, fast_level) + jitter + device_shift


def draw_extra_decay_log(key, part):
    spot_key, loss_key = jax.random.split(jax.random.fold_in(key, 41), 2)
    spot_index = jax.random.randint(spot_key, (HEADS, 3), 0, TOKENS)
    losses = jax.random.uniform(loss_key, (HEADS, 3), jnp.float32, -0.6931, -0.2231)
    head_rows = jnp.broadcast_to(jnp.arange(HEADS)[:, None], (HEADS, 3))
    return jnp.zeros((HEADS, TOKENS), jnp.float32).at[head_rows, spot_index].set(losses)


def levels(own_key, dims, cuts, least, high):
    loudness, own = 1.0, jax.random.fold_in(own_key, 6)
    for dim, blocks in cuts:
        heights = jnp.exp(jax.random.uniform(jax.random.fold_in(own, dim), (blocks,), jnp.float32, least / len(cuts), high / len(cuts)))
        loudness = loudness * jnp.repeat(heights, dims[dim] // blocks).reshape([-1 if axis == dim else 1 for axis in range(len(dims))])
    return loudness


def shared_out(rng, own, number, rows, number_of, top, reach, slope):
    order = jax.random.permutation(rng, number_of)
    crowded, common = shares(number_of, rows * top, reach, slope, True), shares(number_of, rows * top, reach, slope, False)
    places = jnp.arange(number_of)

    def named(sizes, rotation):
        used = int((sizes > 0).sum())
        fixed = max(1, used // 4)
        moved = fixed + (places - fixed + rotation * (used - fixed)) % max(1, number_of - fixed)
        return jnp.zeros((number_of,), jnp.int32).at[order[jnp.where(places < fixed, places, moved)]].set(jnp.asarray(sizes, jnp.int32))

    sizes = jnp.where(number % 4 == 0, named(crowded, number // 4), named(common, number - number // 4 - 1))
    mixed = jax.random.permutation(jax.random.fold_in(own, 3), number_of)
    giver, taker = mixed[0:number_of // 2 * 2:2], mixed[1:number_of // 2 * 2:2]
    slack = jnp.minimum(sizes[giver] - 1, reach - sizes[taker]) // 2
    slack = jnp.where((giver == order[0]) | (taker == order[0]) | (sizes[taker] == 0), 0, jnp.maximum(slack, 0))
    moved = jax.random.randint(jax.random.fold_in(own, 4), (number_of // 2,), 0, 1 << 20) % (slack + 1)
    sizes = sizes.at[giver].add(-moved).at[taker].add(moved)
    members = jnp.searchsorted(jnp.cumsum(sizes), jnp.arange(rows * top), side="right").astype(jnp.int32)
    listing = members.reshape(top, rows).T
    listing = listing[jax.random.permutation(jax.random.fold_in(own, 1), rows)]
    rotation = jax.random.randint(jax.random.fold_in(own, 2), (rows, 1), 0, top)
    return jnp.take_along_axis(listing, (jnp.arange(top)[None, :] + rotation) % top, axis=1)


def shares(count, total, limit, lean, full):
    loads = [(1 << 20) // math.isqrt(grade ** lean) + 1 for grade in range(1, count + 1)]
    largest = limit if full else min(limit, max(-(-total // count), total * loads[0] // sum(loads)))
    least = 1 if total - largest >= count - 1 else 0
    holding, spare = [largest] + [least] * (count - 1), total - largest - least * (count - 1)
    while spare > 0:
        movable = [i for i in range(1, count) if holding[i] < largest] or [i for i in range(1, count) if holding[i] < limit]
        mass, remaining = sum([loads[i] for i in movable]), spare
        for i in movable:
            extra = min(limit - holding[i], max(1, remaining * loads[i] // mass), spare)
            holding[i] = holding[i] + extra
            spare = spare - extra
    return np.array(holding)


def normal_values(stream_key, extent, width, limit, cuts=(), kind=jnp.bfloat16):
    array = width * jax.random.normal(stream_key, extent, jnp.float32)
    if cuts:
        array = array * levels(stream_key, extent, cuts, -0.22, 0.18)
    return jnp.clip(array, -limit, limit).astype(kind)


def setup_inputs(seed: int = 0) -> dict:
    seeds = jax.random.split(jax.random.key(seed), 17)
    queries = normal_values(seeds[0], (TOKENS, HEADS * DQK), 1.0, 6.0, ((0, 8), (1, 4)))
    keys = normal_values(seeds[1], (TOKENS, HEADS * DQK), 1.0, 6.0, ((0, 8), (1, 4)))
    values = normal_values(seeds[2], (TOKENS, HEADS * DV), 1.0, 6.0, ((0, 8), (1, 4)))
    input_gate_log = draw_input_gate_log(jax.random.fold_in(seeds[16], 71), 0)
    forget_gate_logits = draw_forget_gate_logits(jax.random.fold_in(seeds[16], 71), 0)
    extra_decay_log = draw_extra_decay_log(jax.random.fold_in(seeds[16], 71), 0)
    output_gate_logits = normal_values(seeds[6], (TOKENS, HEADS * DV), 1.0, 6.0, ((0, 8), (1, 4)))
    head_norm_scale = jnp.clip(1.0 + 0.18 * jax.random.normal(seeds[7], (HEADS * DV,), jnp.float32), 0.1, 1.9)
    layer_residual_input = normal_values(seeds[8], (TOKENS, D), 1.0, 6.0, ((0, 32),))
    output_projection_weight = normal_values(seeds[9], (HEADS * DV, D), (HEADS * DV) ** -0.5, 0.1875)
    expert_norm_scale = jnp.clip(1.0 + 0.18 * jax.random.normal(seeds[10], (D,), jnp.float32), 0.1, 1.9)
    routing_expert_index_keys = jax.random.split(jax.random.fold_in(seeds[11], 1), TOKENS // ROWS)
    routing_expert_index_turns = jax.random.permutation(jax.random.fold_in(seeds[11], 3), TOKENS // ROWS)
    routing_expert_index = jax.vmap(lambda own, number: shared_out(jax.random.fold_in(seeds[11], 2), own, number, ROWS, EXPERTS, TOP, CAP, 1))(routing_expert_index_keys, routing_expert_index_turns).reshape((TOKENS, TOP))
    routing_expert_weight = jnp.clip(0.2 + 0.8 * jax.random.uniform(seeds[12], (TOKENS, TOP), jnp.float32) ** levels(seeds[12], (TOKENS, TOP), ((0, 32),), -0.2, 0.2), 0.2, 1.0)
    expert_gate_weight = normal_values(seeds[13], (EXPERTS, D, FF), D ** -0.5, 0.125, ((0, 32),))
    expert_up_weight = normal_values(seeds[14], (EXPERTS, D, FF), D ** -0.5, 0.125, ((0, 32),))
    expert_down_weight = normal_values(seeds[15], (EXPERTS, FF, D), FF ** -0.5, 0.1875, ((0, 32),))
    return dict(queries=queries, keys=keys, values=values, input_gate_log=input_gate_log, forget_gate_logits=forget_gate_logits, extra_decay_log=extra_decay_log, output_gate_logits=output_gate_logits, head_norm_scale=head_norm_scale, layer_residual_input=layer_residual_input, output_projection_weight=output_projection_weight, expert_norm_scale=expert_norm_scale, routing_expert_index=routing_expert_index, routing_expert_weight=routing_expert_weight, expert_gate_weight=expert_gate_weight, expert_up_weight=expert_up_weight, expert_down_weight=expert_down_weight)


very_low = -1e+30
epsilon = 1e-06
highest = lax.Precision.HIGHEST

def block_step(carried, inputs):
    memory, stabilizer = carried
    query_blk, key_blk, value_blk, input_blk, forget_blk = inputs
    length = query_blk.shape[1]
    within = jnp.cumsum(forget_blk, axis=-1)
    causal = jnp.arange(length)[:, None] >= jnp.arange(length)[None, :]
    log_weight = jnp.where(causal, within[:, :, None] - within[:, None, :] + input_blk[:, None, :], very_low)
    from_state = within + stabilizer[:, None]
    largest = jnp.maximum(from_state, lax.optimization_barrier(jnp.max(log_weight, axis=-1)))
    intra_weight = jnp.exp(log_weight - largest[:, :, None])
    state_weight = jnp.exp(from_state - largest)
    scores = jnp.einsum('htd,hsd->hts', query_blk, key_blk, precision=highest) * intra_weight
    numerator = jnp.einsum('hts,hsv->htv', scores, value_blk, precision=highest) + state_weight[:, :, None] * jnp.einsum('htd,hdv->htv', query_blk, memory, precision=highest)
    block_total = within[:, -1]
    to_end = block_total[:, None] - within + input_blk
    new_stabilizer = jnp.maximum(block_total + stabilizer, lax.optimization_barrier(jnp.max(to_end, axis=-1)))
    retain = jnp.exp(block_total + stabilizer - new_stabilizer)
    state_add = jnp.exp(to_end - new_stabilizer[:, None])
    memory = retain[:, None, None] * memory + jnp.einsum('hsd,hsv->hdv', key_blk * state_add[:, :, None], value_blk, precision=highest)
    return ((memory, new_stabilizer), numerator)

def reference(queries, keys, values, input_gate_log, forget_gate_logits, extra_decay_log, output_gate_logits, head_norm_scale, layer_residual_input, output_projection_weight, expert_norm_scale, routing_expert_index, routing_expert_weight, expert_gate_weight, expert_up_weight, expert_down_weight):
    blocks = TOKENS // BLOCK

    def to_blocks(matrix, columns):
        return matrix.astype(jnp.float32).reshape(blocks, BLOCK, HEADS, columns).transpose(0, 2, 1, 3)

    def gate_blocks(matrix):
        return matrix.reshape(HEADS, blocks, BLOCK).transpose(1, 0, 2)
    query_blocks = to_blocks(queries, DQK) * DQK ** (-0.5)
    key_blocks = to_blocks(keys, DQK)
    value_blocks = to_blocks(values, DV)
    forget_log_value = jax.nn.log_sigmoid(forget_gate_logits) + extra_decay_log
    initial = (jnp.zeros((HEADS, DQK, DV), jnp.float32), jnp.zeros((HEADS,), jnp.float32))
    unused, numerator = lax.scan(block_step, initial, (query_blocks, key_blocks, value_blocks, gate_blocks(input_gate_log), gate_blocks(forget_log_value)))
    cell_out = numerator.transpose(0, 2, 1, 3).reshape(TOKENS, HEADS, DV)
    scaled = cell_out * lax.rsqrt(lax.optimization_barrier(jnp.mean(cell_out * cell_out, axis=-1, keepdims=True)) + epsilon)
    gated_out = jax.nn.sigmoid(output_gate_logits.astype(jnp.float32)).reshape(TOKENS, HEADS, DV) * scaled * head_norm_scale.reshape(HEADS, DV)
    mixture = gated_out.reshape(TOKENS, HEADS * DV).astype(jnp.bfloat16)
    middle = (layer_residual_input.astype(jnp.float32) + jnp.dot(mixture, output_projection_weight, preferred_element_type=jnp.float32)).astype(jnp.bfloat16)
    middle_wide = middle.astype(jnp.float32)
    normed = (middle_wide * lax.rsqrt(lax.optimization_barrier(jnp.mean(middle_wide * middle_wide, axis=-1, keepdims=True)) + epsilon) * expert_norm_scale).astype(jnp.bfloat16)
    flat_ids = routing_expert_index.reshape(-1)
    flat_weights = routing_expert_weight.reshape(-1)
    most_rows = CAP * N_SP * N_TP

    def one_expert(expert_id, running):
        chosen = flat_ids == expert_id
        picked = jnp.nonzero(chosen, size=most_rows, fill_value=0)[0].astype(jnp.int32)
        in_range = jnp.arange(most_rows) < jnp.sum(chosen)
        token_rows = picked // TOP
        expert_rows = jnp.take(normed, token_rows, axis=0)
        gate_part = jnp.dot(expert_rows, expert_gate_weight[expert_id], preferred_element_type=jnp.float32)
        up_part = jnp.dot(expert_rows, expert_up_weight[expert_id], preferred_element_type=jnp.float32)
        activation = (jax.nn.silu(gate_part) * up_part).astype(jnp.bfloat16)
        produced = jnp.dot(activation, expert_down_weight[expert_id], preferred_element_type=jnp.float32).astype(jnp.bfloat16)
        row_weight = jnp.where(in_range, jnp.take(flat_weights, picked), jnp.float32(0.0))
        return running.at[token_rows].add(row_weight[:, None] * produced.astype(jnp.float32))
    expert_sum = lax.fori_loop(0, EXPERTS, one_expert, jnp.zeros((TOKENS, D), jnp.float32))
    return (middle_wide + expert_sum).astype(jnp.bfloat16)
```

```python
import functools

import jax
import jax.numpy as jnp
from jax import lax
from jax.experimental import pallas as pl
from jax.experimental.pallas import tpu as pltpu
from jax.sharding import PartitionSpec as P

TOP = 2
BLOCK = 128
PLANES = 4


very_low = -1e30
epsilon = 1e-06
MESH = pl.DeviceIdType.MESH


def split(value):
    high = value.astype(jnp.bfloat16)
    return high, (value - high.astype(jnp.float32)).astype(jnp.bfloat16)


def dot_f32(a, b):
    return jnp.dot(a, b, preferred_element_type=jnp.float32)


def along_lanes(value, join, empty):
    lane = lax.broadcasted_iota(jnp.int32, value.shape, 1)
    shift = 1
    while shift < value.shape[1]:
        moved = jnp.where(lane >= shift, pltpu.roll(value, shift, 1), empty)
        value = join(value, moved)
        shift *= 2
    return value


def route_notes(index_ref, weight_ref, experts, slots):
    tokens = index_ref.shape[1]
    expert = lax.broadcasted_iota(jnp.int32, (experts, tokens), 0)
    before = lax.broadcasted_iota(jnp.int32, (tokens, tokens), 0) < lax.broadcasted_iota(
        jnp.int32, (tokens, tokens), 1
    )
    before = jnp.where(before, 1.0, 0.0).astype(jnp.bfloat16)
    base = jnp.zeros((experts, 1), jnp.float32)
    lines = []
    for j in range(TOP):
        row = index_ref[j : j + 1, :]
        named = jnp.where(expert == row, 1.0, 0.0)
        seen = dot_f32(named.astype(jnp.bfloat16), before) + base
        position = jnp.sum(named * seen, axis=0, keepdims=True)
        lines.append(row.astype(jnp.float32) * slots + position)
        base = base + jnp.sum(named, axis=1, keepdims=True)
    lines += [weight_ref[j : j + 1, :] for j in range(TOP)]
    lines.append(jnp.zeros((8 - 2 * TOP, tokens), jnp.float32))
    return jnp.concatenate(lines, axis=0)


def cell_kernel(n, tp_size, heads, experts, slots,
                query_ref, key_ref, value_ref, input_ref, forget_ref, extra_ref, gate_ref,
                head_scale_ref, residual_ref, projection_ref, norm_scale_ref, index_ref, weight_ref,
                middle_ref, normed_ref, notes_ref,
                state, state_notes, got_state, got_notes, carried, intra, mix, token_mix, weights,
                send_state, send_notes, recv_state, recv_notes, send_mix, recv_mix, weight_sem):
    sp = lax.axis_index("sp")
    tp = lax.axis_index("tp")
    length = query_ref.shape[0]
    blocks = length // BLOCK
    keys = query_ref.shape[1] // heads
    wide = value_ref.shape[1] // heads
    share = length // tp_size
    columns = heads * wide

    weight_copy = pltpu.make_async_copy(projection_ref, weights, weight_sem)
    weight_copy.start()
    barrier = pltpu.get_barrier_semaphore()

    def greet_sp(k, carry):
        pl.semaphore_signal(
            barrier, inc=1, device_id={"sp": lax.rem(sp + k, n)}, device_id_type=MESH
        )
        return carry

    lax.fori_loop(1, n, greet_sp, 0)
    for k in range(1, tp_size):
        pl.semaphore_signal(
            barrier, inc=1, device_id={"tp": lax.rem(tp + k, tp_size)}, device_id_type=MESH
        )

    def state_copies(source, target):
        kind = dict(device_id={"sp": target}, device_id_type=MESH)
        return (
            pltpu.make_async_remote_copy(
                src_ref=state, dst_ref=got_state.at[source],
                send_sem=send_state.at[target], recv_sem=recv_state.at[source], **kind),
            pltpu.make_async_remote_copy(
                src_ref=state_notes, dst_ref=got_notes.at[source],
                send_sem=send_notes.at[target], recv_sem=recv_notes.at[source], **kind),
        )

    def mix_copy(source, target):
        return pltpu.make_async_remote_copy(
            src_ref=mix.at[pl.ds(target * share, share), :],
            dst_ref=token_mix.at[:, pl.ds(pl.multiple_of(source * columns, columns), columns)],
            send_sem=send_mix.at[target], recv_sem=recv_mix.at[source],
            device_id={"tp": target}, device_id_type=MESH)

    def by_block(value):
        return jnp.concatenate(
            [value[h : h + 1, b * BLOCK : (b + 1) * BLOCK]
             for h in range(heads) for b in range(blocks)], axis=0)

    logits = forget_ref[...]
    decay = jnp.minimum(logits, 0.0) - jnp.log1p(jnp.exp(-jnp.abs(logits))) + extra_ref[...]
    within = along_lanes(by_block(decay), jnp.add, 0.0)
    level = by_block(input_ref[...]) - within
    peak = along_lanes(level, jnp.maximum, very_low)
    total = within[:, BLOCK - 1 : BLOCK]
    top = peak[:, BLOCK - 1 : BLOCK]
    state_add = jnp.exp(level - top)
    block_max = total + top
    largest = within + peak

    keys_t = key_ref[...].astype(jnp.float32).T
    keys_t_low = keys_t.astype(jnp.bfloat16)
    zero = jnp.zeros((1, 1), jnp.float32)
    state_notes[...] = jnp.zeros_like(state_notes)
    local_max, local_before = [], []
    for h in range(heads):
        memory = jnp.zeros((keys, wide), jnp.float32)
        high_mark = jnp.full((1, 1), very_low, jnp.float32)
        passed = zero
        for b in range(blocks):
            row = h * blocks + b
            carried[row] = memory
            local_max.append(high_mark)
            local_before.append(passed)
            added_high, added_low = split(
                keys_t[h * keys : (h + 1) * keys, b * BLOCK : (b + 1) * BLOCK]
                * state_add[row : row + 1, :]
            )
            values = value_ref[b * BLOCK : (b + 1) * BLOCK, h * wide : (h + 1) * wide]
            added = dot_f32(added_high, values) + dot_f32(added_low, values)
            shifted = high_mark + total[row : row + 1]
            combined = jnp.maximum(shifted, block_max[row : row + 1])
            memory = jnp.exp(shifted - combined) * memory + jnp.exp(
                block_max[row : row + 1] - combined
            ) * added
            high_mark = combined
            passed = passed + total[row : row + 1]
        state[h * keys : (h + 1) * keys, :] = memory.astype(jnp.bfloat16)
        state_notes[h : h + 1, :] = jnp.broadcast_to(passed, (1, wide))
        state_notes[heads + h : heads + h + 1, :] = jnp.broadcast_to(high_mark, (1, wide))
    pl.semaphore_wait(barrier, n + tp_size - 2)

    def send_on(k, carry):
        @pl.when(sp + k < n)
        def _():
            for copy in state_copies(sp, sp + k):
                copy.start()

        return carry

    lax.fori_loop(1, n, send_on, 0)

    notes_ref[...] = route_notes(index_ref, weight_ref, experts, slots)
    causal = lax.broadcasted_iota(jnp.int32, (BLOCK, BLOCK), 0) >= lax.broadcasted_iota(
        jnp.int32, (BLOCK, BLOCK), 1
    )
    lane = lax.broadcasted_iota(jnp.int32, (BLOCK, heads * keys), 1)
    peak_t = peak.T

    def own_query(h, b):
        query = query_ref[b * BLOCK : (b + 1) * BLOCK, :] * jnp.bfloat16(keys ** -0.5)
        return jnp.where(
            (lane >= h * keys) & (lane < (h + 1) * keys), query, jnp.zeros_like(query)
        )

    for h in range(heads):
        for b in range(blocks):
            row = h * blocks + b
            scores = dot_f32(own_query(h, b), keys_t_low[:, b * BLOCK : (b + 1) * BLOCK])
            weight = jnp.exp(
                jnp.where(causal, level[row : row + 1, :] - peak_t[:, row : row + 1], very_low)
            )
            score_high, score_low = split(scores * weight)
            values = value_ref[b * BLOCK : (b + 1) * BLOCK, h * wide : (h + 1) * wide]
            intra[row] = dot_f32(score_high, values) + dot_f32(score_low, values)

    def lap(j, carry):
        memory, marks = carry
        for copy in state_copies(j, sp):
            copy.wait_recv()
        memories, later = [], []
        for h in range(heads):
            passed = got_notes[j, h : h + 1, :]
            late = got_notes[j, heads + h : heads + h + 1, :]
            shifted = passed + marks[h : h + 1, :]
            combined = jnp.maximum(shifted, late)
            memories.append(
                jnp.exp(shifted - combined) * memory[h * keys : (h + 1) * keys, :]
                + jnp.exp(late - combined)
                * got_state[j, h * keys : (h + 1) * keys, :].astype(jnp.float32)
            )
            later.append(combined)
        return jnp.concatenate(memories, axis=0), jnp.concatenate(later, axis=0)

    earlier, marks = lax.fori_loop(
        0, sp, lap,
        (jnp.zeros((heads * keys, wide), jnp.float32), jnp.zeros((heads, wide), jnp.float32)),
    )

    local_marks = jnp.concatenate(local_max, axis=0)
    moved_marks = jnp.concatenate(local_before, axis=0) + jnp.concatenate(
        [marks[h : h + 1, 0:1] for h in range(heads) for _ in range(blocks)], axis=0
    )
    start_marks = jnp.maximum(moved_marks, local_marks)
    moved_scale = jnp.exp(moved_marks - start_marks)
    local_scale = jnp.exp(local_marks - start_marks)
    from_start = within + start_marks
    joined = jnp.maximum(largest, from_start)
    scales = jnp.concatenate(
        [jnp.exp(largest - joined), jnp.exp(from_start - joined)], axis=0
    ).T
    rows = heads * blocks

    for b in range(blocks):
        for h in range(heads):
            row = h * blocks + b
            start = (
                moved_scale[row : row + 1] * earlier[h * keys : (h + 1) * keys, :]
                + local_scale[row : row + 1] * carried[row]
            )
            start_high, start_low = split(start)
            query = query_ref[b * BLOCK : (b + 1) * BLOCK, h * keys : (h + 1) * keys]
            query = query * jnp.bfloat16(keys ** -0.5)
            cell = scales[:, row : row + 1] * intra[row] + scales[
                :, rows + row : rows + row + 1
            ] * (dot_f32(query, start_high) + dot_f32(query, start_low))
            norm = lax.rsqrt(jnp.mean(cell * cell, axis=-1, keepdims=True) + epsilon)
            gate = jax.nn.sigmoid(
                gate_ref[b * BLOCK : (b + 1) * BLOCK, h * wide : (h + 1) * wide].astype(jnp.float32)
            )
            mix[b * BLOCK : (b + 1) * BLOCK, h * wide : (h + 1) * wide] = (
                gate * cell * norm * head_scale_ref[:, h * wide : (h + 1) * wide]
            ).astype(jnp.bfloat16)
        for target in range(tp_size):
            if b == ((target + 1) * share - 1) // BLOCK:
                @pl.when(tp != target)
                def _(target=target):
                    mix_copy(tp, target).start()

    token_mix[:, pl.ds(pl.multiple_of(tp * columns, columns), columns)] = mix[
        pl.ds(pl.multiple_of(tp * share, share), share), :
    ]
    weight_copy.wait()
    for k in range(1, tp_size):
        mix_copy(lax.rem(tp + k, tp_size), tp).wait_recv()
    width = weights.shape[1]
    tile = 256

    def project(t, squares):
        where = pl.ds(pl.multiple_of(t * tile, tile), tile)
        middle = (
            residual_ref[:, where].astype(jnp.float32)
            + dot_f32(token_mix[...], weights[:, where])
        ).astype(jnp.bfloat16)
        middle_ref[:, where] = middle
        middle = middle.astype(jnp.float32)
        return squares + jnp.sum(middle * middle, axis=-1, keepdims=True)

    squares = lax.fori_loop(
        0, width // tile, project, jnp.zeros((share, 1), jnp.float32)
    )
    norm = lax.rsqrt(squares * (1.0 / width) + epsilon)

    def scale_rows(t, carry):
        where = pl.ds(pl.multiple_of(t * tile, tile), tile)
        normed_ref[:, where] = (
            middle_ref[:, where].astype(jnp.float32) * norm * norm_scale_ref[:, where]
        ).astype(jnp.bfloat16)
        return carry

    lax.fori_loop(0, width // tile, scale_rows, 0)

    def finish(k, carry):
        @pl.when(sp + k < n)
        def _():
            for copy in state_copies(sp, sp + k):
                copy.wait_send()

        return carry

    lax.fori_loop(1, n, finish, 0)
    for k in range(1, tp_size):
        mix_copy(tp, lax.rem(tp + k, tp_size)).wait_send()


def cell_call(heads, experts, slots, arrays):
    queries, values, residual, projection = arrays[0], arrays[2], arrays[8], arrays[9]
    n = lax.axis_size("sp")
    tp_size = lax.axis_size("tp")
    length = queries.shape[0]
    keys = queries.shape[1] // heads
    wide = values.shape[1] // heads
    rows = heads * (length // BLOCK)
    tokens, width = residual.shape
    note_rows = -(-2 * heads // 8) * 8
    vmem = pl.BlockSpec(memory_space=pltpu.VMEM)
    anywhere = pl.BlockSpec(memory_space=pl.ANY)
    dma = pltpu.SemaphoreType.DMA
    specs = [vmem] * len(arrays)
    specs[9] = anywhere
    return pl.pallas_call(
        functools.partial(cell_kernel, n, tp_size, heads, experts, slots),
        out_shape=(
            jax.ShapeDtypeStruct((tokens, width), jnp.bfloat16),
            jax.ShapeDtypeStruct((tokens, width), jnp.bfloat16),
            jax.ShapeDtypeStruct((8, tokens), jnp.float32),
        ),
        in_specs=specs,
        out_specs=(vmem, vmem, vmem),
        scratch_shapes=[
            pltpu.VMEM((heads * keys, wide), jnp.bfloat16),
            pltpu.VMEM((note_rows, wide), jnp.float32),
            pltpu.VMEM((n, heads * keys, wide), jnp.bfloat16),
            pltpu.VMEM((n, note_rows, wide), jnp.float32),
            pltpu.VMEM((rows, keys, wide), jnp.float32),
            pltpu.VMEM((rows, BLOCK, wide), jnp.float32),
            pltpu.VMEM((length, heads * wide), jnp.bfloat16),
            pltpu.VMEM((tokens, projection.shape[0]), jnp.bfloat16),
            pltpu.VMEM(projection.shape, jnp.bfloat16),
            dma((n,)), dma((n,)), dma((n,)), dma((n,)),
            dma((tp_size,)), dma((tp_size,)),
            dma(()),
        ],
        compiler_params=pltpu.CompilerParams(collective_id=0, has_side_effects=True),
    )(*arrays)


def expert_kernel(tp_size, chunks, tile,
                  normed_ref, middle_ref, notes_ref, gate_ref, up_ref, down_ref, out_ref,
                  notes, rows, sent, arrived, produced, returned, outcome,
                  activation, gate_w, up_w, down_w,
                  notes_send, notes_recv, rows_send, rows_recv, there_send, there_recv,
                  back_send, back_recv, weight_sems):
    sp = lax.axis_index("sp")
    tp = lax.axis_index("tp")
    lanes, part = rows.shape[2:]
    halves, members, slots, wide = sent.shape[1:]
    each = chunks // halves
    width = halves * wide
    hidden = gate_w.shape[1]
    sp_rows = members // tp_size
    plane = sp // sp_rows
    member = lax.rem(sp, sp_rows) * tp_size + tp
    last = PLANES - 1
    upper = plane >= PLANES // 2
    outward = jnp.where(upper, 1, -1)
    at_end = (plane == 0) | (plane == last)

    def place(to_plane, to_member):
        return dict(
            device_id={"sp": to_plane * sp_rows + to_member // tp_size,
                       "tp": lax.rem(to_member, tp_size)},
            device_id_type=MESH,
        )

    def beside(step):
        return lax.rem(plane + step + PLANES, PLANES)

    weight_copies = [
        pltpu.make_async_copy(source.at[0], target, weight_sems.at[k])
        for k, (source, target) in enumerate(
            ((gate_ref, gate_w), (up_ref, up_w), (down_ref, down_w))
        )
    ]
    for copy in weight_copies:
        copy.start()

    barrier = pltpu.get_barrier_semaphore()
    for k in range(1, members):
        pl.semaphore_signal(barrier, inc=1, **place(plane, lax.rem(member + k, members)))
    for k in range(1, PLANES):
        pl.semaphore_signal(barrier, inc=1, **place(beside(k), member))
    pl.semaphore_wait(barrier, members + PLANES - 2)

    def notes_copy(source, target):
        return pltpu.make_async_remote_copy(
            src_ref=notes_ref, dst_ref=notes.at[source],
            send_sem=notes_send.at[target], recv_sem=notes_recv.at[source],
            **place(target, member))

    def rows_copy(block, k, step, own=False):
        source = normed_ref.at[:, pl.ds(k * part, part)] if own else rows.at[block, k]
        return pltpu.make_async_remote_copy(
            src_ref=source, dst_ref=rows.at[block, k],
            send_sem=rows_send.at[(step + 1) // 2, block, k], recv_sem=rows_recv.at[block, k],
            **place(beside(step), member))

    def there(block, half, target):
        return pltpu.make_async_remote_copy(
            src_ref=sent.at[block, half, target], dst_ref=arrived.at[block, half, member],
            send_sem=there_send.at[block, half], recv_sem=there_recv.at[block, half],
            **place(plane, target))

    def back(block, half, target):
        return pltpu.make_async_remote_copy(
            src_ref=produced.at[block, half, target],
            dst_ref=returned.at[plane, half, member],
            send_sem=back_send.at[block, half], recv_sem=back_recv.at[plane, half],
            **place(block, target))

    def bytes_of(buffer, block, half, sem, count):
        span = buffer.at[block, half, pl.ds(0, count)]
        return pltpu.make_async_copy(span, span, sem.at[block, half])

    for k in range(1, PLANES):
        notes_copy(plane, beside(k)).start()
    for step in (1, -1):
        @pl.when((plane + step >= 0) & (plane + step <= last))
        def _(step=step):
            for k in range(chunks):
                rows_copy(plane, k, step, True).start()
    notes[plane] = notes_ref[...]
    for k in range(chunks):
        rows[plane, k] = normed_ref[:, k * part : (k + 1) * part]

    def matches(block, of_plane):
        slot = lax.broadcasted_iota(jnp.int32, (members * slots, lanes), 0)
        slot = (slot + of_plane * (members * slots)).astype(jnp.float32)
        return notes[block, 0:1, :] == slot, notes[block, 1:2, :] == slot

    def dispatch(block, half):
        first, second = matches(block, plane)
        pick = jnp.where(first | second, 1.0, 0.0).astype(jnp.bfloat16)
        for k in range(each):
            chosen = dot_f32(pick, rows[block, half * each + k]).astype(jnp.bfloat16)
            sent[block, half, :, :, k * part : (k + 1) * part] = chosen.reshape(
                members, slots, part
            )
        for i in range(1, members):
            there(block, half, lax.rem(member + i, members)).start()
        arrived[block, half, member] = sent[block, half, member]

    def take(block, half, forward):
        for k in range(half * each, (half + 1) * each):
            rows_copy(block, k, -1).wait_recv()
            if forward is not None:
                rows_copy(block, k, forward).start()
        dispatch(block, half)

    def give_back(block, half):
        for i in range(1, members):
            back(block, half, lax.rem(member + i, members)).start()
        back(block, half, member).start()

    def give_home():
        for half in range(halves):
            for i in range(1, members):
                back(plane, half, lax.rem(member + i, members)).start()
            returned[plane, half, member] = produced[plane, half, member]

    def give_late(block):
        for half in range(halves):
            give_back(block, half)

    def compute(block, send=True):
        for half in range(halves):
            bytes_of(arrived, block, half, there_recv, members - 1).wait()

        def hidden_tile(t, carry):
            columns = pl.ds(pl.multiple_of(t * tile, tile), tile)
            gate_part = up_part = 0.0
            for half in range(halves):
                tokens = arrived[block, half].reshape(members * slots, wide)
                span = slice(half * wide, (half + 1) * wide)
                gate_part = gate_part + dot_f32(tokens, gate_w[span, columns])
                up_part = up_part + dot_f32(tokens, up_w[span, columns])
            activation[:, columns] = (jax.nn.silu(gate_part) * up_part).astype(jnp.bfloat16)
            return carry

        lax.fori_loop(0, hidden // tile, hidden_tile, 0)
        for half in range(halves):
            def width_tile(t, carry):
                start = pl.multiple_of(t * tile, tile)
                result = dot_f32(
                    activation[...], down_w[:, pl.ds(half * wide + start, tile)]
                ).astype(jnp.bfloat16)
                produced[block, half, :, :, pl.ds(start, tile)] = result.reshape(
                    members, slots, tile
                )
                return carry

            lax.fori_loop(0, wide // tile, width_tile, 0)
            if send:
                give_back(block, half)


    def gather(of_plane, home=False):
        first, second = matches(plane, of_plane)
        spread = jnp.where(first, notes[plane, 2:3, :], 0.0) + jnp.where(
            second, notes[plane, 3:4, :], 0.0
        )
        high, low = split(spread.T)
        for half in range(halves):
            bytes_of(returned, of_plane, half, back_recv, members - 1 if home else members).wait()
            for k in range(each):
                share = returned[of_plane, half, :, :, k * part : (k + 1) * part].reshape(
                    members * slots, part
                )
                columns = slice(half * wide + k * part, half * wide + (k + 1) * part)
                before = middle_ref[:, columns].astype(jnp.float32) if home else outcome[:, columns]
                outcome[:, columns] = before + dot_f32(high, share) + dot_f32(low, share)

    for half in range(halves):
        dispatch(plane, half)
    for k in range(1, PLANES):
        notes_copy(beside(k), plane).wait_recv()

    @pl.when(at_end)
    def _():
        one, two, three = plane - outward, plane - 2 * outward, plane - 3 * outward
        take(one, 0, None)
        take(one, 1, None)
        for copy in weight_copies:
            copy.wait()
        compute(plane, False)
        compute(one)
        take(two, 0, None)
        take(two, 1, None)
        give_home()
        compute(two)
        take(three, 0, None)
        take(three, 1, None)
        compute(three)
        gather(plane, True)
        gather(one)
        gather(two)
        gather(three)

    @pl.when(jnp.logical_not(at_end))
    def _():
        inner, outer, far = plane - outward, plane + outward, plane - 2 * outward
        take(inner, 0, outward)
        take(outer, 0, -outward)
        take(inner, 1, outward)
        take(outer, 1, -outward)
        for copy in weight_copies:
            copy.wait()
        compute(plane, False)
        compute(inner)
        take(far, 0, outward)
        take(far, 1, outward)
        compute(outer)
        compute(far)
        give_home()
        gather(plane, True)
        gather(outer)
        gather(inner)
        gather(far)

    out_ref[...] = outcome[...].astype(jnp.bfloat16)
    for k in range(1, PLANES):
        notes_copy(plane, beside(k)).wait_send()

    def finish(block, carry):
        @pl.when((block <= plane) & (plane < last))
        def _():
            for k in range(chunks):
                rows_copy(block, k, 1).wait_send()

        @pl.when((block >= plane) & (plane > 0))
        def _():
            for k in range(chunks):
                rows_copy(block, k, -1).wait_send()

        for half in range(halves):
            bytes_of(sent, block, half, there_send, members - 1).wait()
            bytes_of(produced, block, half, back_send, members - 1).wait()

        @pl.when(block != plane)
        def _():
            for half in range(halves):
                bytes_of(produced, block, half, back_send, 1).wait()

        return carry

    lax.fori_loop(0, PLANES, finish, 0)


def expert_call(normed, middle, notes, gate, up, down, slots):
    tokens, width = normed.shape
    hidden = gate.shape[2]
    tp_size = lax.axis_size("tp")
    members = lax.axis_size("sp") * tp_size // PLANES
    chunks, halves = 4, 2
    part = width // chunks
    vmem = pl.BlockSpec(memory_space=pltpu.VMEM)
    anywhere = pl.BlockSpec(memory_space=pl.ANY)
    slotted = pltpu.VMEM((PLANES, halves, members, slots, width // halves), jnp.bfloat16)
    chunked = pltpu.VMEM((PLANES, chunks, tokens, part), jnp.bfloat16)
    dma = pltpu.SemaphoreType.DMA
    return pl.pallas_call(
        functools.partial(expert_kernel, tp_size, chunks, 256),
        out_shape=jax.ShapeDtypeStruct(middle.shape, jnp.bfloat16),
        in_specs=[vmem, vmem, vmem, anywhere, anywhere, anywhere],
        out_specs=vmem,
        scratch_shapes=[
            pltpu.VMEM((PLANES,) + notes.shape, jnp.float32),
            chunked,
            slotted,
            slotted,
            slotted,
            slotted,
            pltpu.VMEM((tokens, width), jnp.float32),
            pltpu.VMEM((members * slots, hidden), jnp.bfloat16),
            pltpu.VMEM((width, hidden), jnp.bfloat16),
            pltpu.VMEM((width, hidden), jnp.bfloat16),
            pltpu.VMEM((hidden, width), jnp.bfloat16),
            dma((PLANES,)),
            dma((PLANES,)),
            dma((2, PLANES, chunks)),
            dma((PLANES, chunks)),
            dma((PLANES, halves)),
            dma((PLANES, halves)),
            dma((PLANES, halves)),
            dma((PLANES, halves)),
            dma((3,)),
        ],
        compiler_params=pltpu.CompilerParams(collective_id=1, has_side_effects=True),
    )(normed, middle, notes, gate, up, down)


def shards(
    queries,
    keys,
    values,
    input_gate_log,
    forget_gate_logits,
    extra_decay_log,
    output_gate_logits,
    head_norm_scale,
    layer_residual_input,
    output_projection_weight,
    expert_norm_scale,
    routing_expert_index,
    routing_expert_weight,
    expert_gate_weight,
    expert_up_weight,
    expert_down_weight,
):
    sp_count = lax.axis_size("sp")
    tp_count = lax.axis_size("tp")
    devices = sp_count * tp_count
    local_experts = expert_gate_weight.shape[0]
    experts = local_experts * devices
    tok_count, model_width = layer_residual_input.shape
    slots = max(2, 2 * tok_count * TOP // experts)
    middle, normed, notes = cell_call(
        input_gate_log.shape[0], experts, slots,
        [
            queries, keys, values, input_gate_log, forget_gate_logits, extra_decay_log,
            output_gate_logits, head_norm_scale[None], layer_residual_input,
            output_projection_weight, expert_norm_scale[None], routing_expert_index.T,
            routing_expert_weight.T,
        ],
    )
    if (
        local_experts == 1
        and slots % 16 == 0
        and sp_count % PLANES == 0
        and model_width % 1024 == 0
    ):
        return expert_call(
            normed, middle, notes, expert_gate_weight, expert_up_weight, expert_down_weight, slots
        )
    slot_key = notes[:TOP].T.astype(jnp.int32).reshape(-1)
    matches = slot_key[None, :] == jnp.arange(experts * slots, dtype=jnp.int32)[:, None]
    pick = jnp.sum(
        matches.reshape(experts * slots, tok_count, TOP).astype(jnp.float32), axis=2
    ).astype(jnp.bfloat16)
    outgoing = (
        jnp.dot(pick, normed, preferred_element_type=jnp.float32)
        .astype(jnp.bfloat16)
        .reshape(experts, slots, model_width)
    )
    weight_high = lax.reduce_precision(routing_expert_weight, 8, 7)
    slot_pairs = slot_key.reshape(tok_count, TOP, 1)
    slot_range = jnp.arange(experts * slots, dtype=jnp.int32)

    def spread(weights):
        return jnp.sum(
            jnp.where(slot_pairs == slot_range, weights[:, :, None], 0.0), axis=1
        ).astype(jnp.bfloat16)

    high = spread(weight_high)
    low = spread(routing_expert_weight - weight_high)
    arrived = lax.all_to_all(outgoing, ("sp", "tp"), split_axis=0, concat_axis=0, tiled=True)
    grouped = arrived.reshape(devices, local_experts, arrived.shape[1], model_width)
    gate_part = jnp.einsum(
        "sxcd,xdf->sxcf", grouped, expert_gate_weight, preferred_element_type=jnp.float32
    )
    up_part = jnp.einsum(
        "sxcd,xdf->sxcf", grouped, expert_up_weight, preferred_element_type=jnp.float32
    )
    activation = (jax.nn.silu(gate_part) * up_part).astype(jnp.bfloat16)
    produced = jnp.einsum(
        "sxcf,xfd->sxcd", activation, expert_down_weight, preferred_element_type=jnp.float32
    ).astype(jnp.bfloat16)
    returned = lax.all_to_all(
        produced.reshape(arrived.shape), ("sp", "tp"), split_axis=0, concat_axis=0, tiled=True
    )
    returned = returned.reshape(experts * slots, model_width)
    expert_sum = jnp.dot(high, returned, preferred_element_type=jnp.float32) + jnp.dot(
        low, returned, preferred_element_type=jnp.float32
    )
    return (middle.astype(jnp.float32) + expert_sum).astype(jnp.bfloat16)


def solution(mesh):
    in_specs = (
        P("sp", "tp"),
        P("sp", "tp"),
        P("sp", "tp"),
        P("tp", "sp"),
        P("tp", "sp"),
        P("tp", "sp"),
        P("sp", "tp"),
        P("tp"),
        P(("sp", "tp"), None),
        P(),
        P(),
        P(("sp", "tp"), None),
        P(("sp", "tp"), None),
        P(("sp", "tp"), None, None),
        P(("sp", "tp"), None, None),
        P(("sp", "tp"), None, None),
    )
    out_specs = P(("sp", "tp"), None)
    return jax.shard_map(shards, mesh=mesh, in_specs=in_specs, out_specs=out_specs, check_vma=False)
```

```python
import functools

import jax
import jax.numpy as jnp
from jax import lax
from jax.experimental import pallas as pl
from jax.experimental.pallas import tpu as pltpu
from jax.sharding import PartitionSpec as P

TOP = 2
BLOCK = 128
PLANES = 4


very_low = -1e30
epsilon = 1e-06
MESH = pl.DeviceIdType.MESH


def split(value):
    high = value.astype(jnp.bfloat16)
    return high, (value - high.astype(jnp.float32)).astype(jnp.bfloat16)


def dot_f32(a, b):
    return jnp.dot(a, b, preferred_element_type=jnp.float32)


def along_lanes(value, join, empty):
    lane = lax.broadcasted_iota(jnp.int32, value.shape, 1)
    shift = 1
    while shift < value.shape[1]:
        moved = jnp.where(lane >= shift, pltpu.roll(value, shift, 1), empty)
        value = join(value, moved)
        shift *= 2
    return value


def route_notes(index_ref, weight_ref, experts, slots):
    tokens = index_ref.shape[1]
    expert = lax.broadcasted_iota(jnp.int32, (experts, tokens), 0)
    before = lax.broadcasted_iota(jnp.int32, (tokens, tokens), 0) < lax.broadcasted_iota(
        jnp.int32, (tokens, tokens), 1
    )
    before = jnp.where(before, 1.0, 0.0).astype(jnp.bfloat16)
    base = jnp.zeros((experts, 1), jnp.float32)
    lines = []
    for j in range(TOP):
        row = index_ref[j : j + 1, :]
        named = jnp.where(expert == row, 1.0, 0.0)
        seen = dot_f32(named.astype(jnp.bfloat16), before) + base
        position = jnp.sum(named * seen, axis=0, keepdims=True)
        lines.append(row.astype(jnp.float32) * slots + position)
        base = base + jnp.sum(named, axis=1, keepdims=True)
    lines += [weight_ref[j : j + 1, :] for j in range(TOP)]
    lines.append(jnp.zeros((8 - 2 * TOP, tokens), jnp.float32))
    return jnp.concatenate(lines, axis=0)


def cell_body(n, tp_size, heads, experts, slots, inputs, scratch, barrier_count, announce, publish):
    (query_ref, key_ref, value_ref, input_ref, forget_ref, extra_ref, gate_ref, head_scale_ref,
     residual_ref, projection_ref, norm_scale_ref, index_ref, weight_ref) = inputs
    (notes_ref, outcome, state, state_notes, got_state, got_notes, carried, intra, mix, token_mix,
     weights, send_state, send_notes, recv_state, recv_notes, send_mix, recv_mix,
     weight_sem) = scratch
    sp = lax.axis_index("sp")
    tp = lax.axis_index("tp")
    length = query_ref.shape[0]
    blocks = length // BLOCK
    keys = query_ref.shape[1] // heads
    wide = value_ref.shape[1] // heads
    share = length // tp_size
    columns = heads * wide

    weight_copy = pltpu.make_async_copy(projection_ref, weights, weight_sem)
    weight_copy.start()
    barrier = pltpu.get_barrier_semaphore()

    def state_copies(source, target):
        kind = dict(device_id={"sp": target}, device_id_type=MESH)
        return (
            pltpu.make_async_remote_copy(
                src_ref=state, dst_ref=got_state.at[source],
                send_sem=send_state.at[target], recv_sem=recv_state.at[source], **kind),
            pltpu.make_async_remote_copy(
                src_ref=state_notes, dst_ref=got_notes.at[source],
                send_sem=send_notes.at[target], recv_sem=recv_notes.at[source], **kind),
        )

    def mix_copy(source, target):
        return pltpu.make_async_remote_copy(
            src_ref=mix.at[pl.ds(target * share, share), :],
            dst_ref=token_mix.at[:, pl.ds(pl.multiple_of(source * columns, columns), columns)],
            send_sem=send_mix.at[target], recv_sem=recv_mix.at[source],
            device_id={"tp": target}, device_id_type=MESH)

    def by_block(value):
        return jnp.concatenate(
            [value[h : h + 1, b * BLOCK : (b + 1) * BLOCK]
             for h in range(heads) for b in range(blocks)], axis=0)

    logits = forget_ref[...]
    decay = jnp.minimum(logits, 0.0) - jnp.log1p(jnp.exp(-jnp.abs(logits))) + extra_ref[...]
    within = along_lanes(by_block(decay), jnp.add, 0.0)
    level = by_block(input_ref[...]) - within
    peak = along_lanes(level, jnp.maximum, very_low)
    total = within[:, BLOCK - 1 : BLOCK]
    top = peak[:, BLOCK - 1 : BLOCK]
    state_add = jnp.exp(level - top)
    block_max = total + top
    largest = within + peak

    keys_t = key_ref[...].astype(jnp.float32).T
    keys_t_low = keys_t.astype(jnp.bfloat16)
    zero = jnp.zeros((1, 1), jnp.float32)
    state_notes[...] = jnp.zeros_like(state_notes)
    local_max, local_before = [], []
    for h in range(heads):
        memory = jnp.zeros((keys, wide), jnp.float32)
        high_mark = jnp.full((1, 1), very_low, jnp.float32)
        passed = zero
        for b in range(blocks):
            row = h * blocks + b
            carried[row] = memory
            local_max.append(high_mark)
            local_before.append(passed)
            added_high, added_low = split(
                keys_t[h * keys : (h + 1) * keys, b * BLOCK : (b + 1) * BLOCK]
                * state_add[row : row + 1, :]
            )
            values = value_ref[b * BLOCK : (b + 1) * BLOCK, h * wide : (h + 1) * wide]
            added = dot_f32(added_high, values) + dot_f32(added_low, values)
            shifted = high_mark + total[row : row + 1]
            combined = jnp.maximum(shifted, block_max[row : row + 1])
            memory = jnp.exp(shifted - combined) * memory + jnp.exp(
                block_max[row : row + 1] - combined
            ) * added
            high_mark = combined
            passed = passed + total[row : row + 1]
        state[h * keys : (h + 1) * keys, :] = memory.astype(jnp.bfloat16)
        state_notes[h : h + 1, :] = jnp.broadcast_to(passed, (1, wide))
        state_notes[heads + h : heads + h + 1, :] = jnp.broadcast_to(high_mark, (1, wide))
    pl.semaphore_wait(barrier, barrier_count)

    def send_on(k, carry):
        @pl.when(sp + n - k < n)
        def _():
            for copy in state_copies(sp, sp + n - k):
                copy.start()

        return carry

    lax.fori_loop(1, n, send_on, 0)

    notes_ref[...] = route_notes(index_ref, weight_ref, experts, slots)
    announce()
    causal = lax.broadcasted_iota(jnp.int32, (BLOCK, BLOCK), 0) >= lax.broadcasted_iota(
        jnp.int32, (BLOCK, BLOCK), 1
    )
    lane = lax.broadcasted_iota(jnp.int32, (BLOCK, heads * keys), 1)
    peak_t = peak.T

    def own_query(h, b):
        query = query_ref[b * BLOCK : (b + 1) * BLOCK, :] * jnp.bfloat16(keys ** -0.5)
        return jnp.where(
            (lane >= h * keys) & (lane < (h + 1) * keys), query, jnp.zeros_like(query)
        )

    for h in range(heads):
        for b in range(blocks):
            row = h * blocks + b
            scores = dot_f32(own_query(h, b), keys_t_low[:, b * BLOCK : (b + 1) * BLOCK])
            weight = jnp.exp(
                jnp.where(causal, level[row : row + 1, :] - peak_t[:, row : row + 1], very_low)
            )
            score_high, score_low = split(scores * weight)
            values = value_ref[b * BLOCK : (b + 1) * BLOCK, h * wide : (h + 1) * wide]
            intra[row] = dot_f32(score_high, values) + dot_f32(score_low, values)

    def lap(j, carry):
        memory, marks = carry
        for copy in state_copies(j, sp):
            copy.wait_recv()
        memories, later = [], []
        for h in range(heads):
            passed = got_notes[j, h : h + 1, :]
            late = got_notes[j, heads + h : heads + h + 1, :]
            shifted = passed + marks[h : h + 1, :]
            combined = jnp.maximum(shifted, late)
            memories.append(
                jnp.exp(shifted - combined) * memory[h * keys : (h + 1) * keys, :]
                + jnp.exp(late - combined)
                * got_state[j, h * keys : (h + 1) * keys, :].astype(jnp.float32)
            )
            later.append(combined)
        return jnp.concatenate(memories, axis=0), jnp.concatenate(later, axis=0)

    earlier, marks = lax.fori_loop(
        0, sp, lap,
        (jnp.zeros((heads * keys, wide), jnp.float32), jnp.zeros((heads, wide), jnp.float32)),
    )

    local_marks = jnp.concatenate(local_max, axis=0)
    moved_marks = jnp.concatenate(local_before, axis=0) + jnp.concatenate(
        [marks[h : h + 1, 0:1] for h in range(heads) for _ in range(blocks)], axis=0
    )
    start_marks = jnp.maximum(moved_marks, local_marks)
    moved_scale = jnp.exp(moved_marks - start_marks)
    local_scale = jnp.exp(local_marks - start_marks)
    from_start = within + start_marks
    joined = jnp.maximum(largest, from_start)
    scales = jnp.concatenate(
        [jnp.exp(largest - joined), jnp.exp(from_start - joined)], axis=0
    ).T
    rows = heads * blocks

    for b in range(blocks):
        for h in range(heads):
            row = h * blocks + b
            start = (
                moved_scale[row : row + 1] * earlier[h * keys : (h + 1) * keys, :]
                + local_scale[row : row + 1] * carried[row]
            )
            start_high, start_low = split(start)
            query = query_ref[b * BLOCK : (b + 1) * BLOCK, h * keys : (h + 1) * keys]
            query = query * jnp.bfloat16(keys ** -0.5)
            cell = scales[:, row : row + 1] * intra[row] + scales[
                :, rows + row : rows + row + 1
            ] * (dot_f32(query, start_high) + dot_f32(query, start_low))
            norm = lax.rsqrt(jnp.mean(cell * cell, axis=-1, keepdims=True) + epsilon)
            gate = jax.nn.sigmoid(
                gate_ref[b * BLOCK : (b + 1) * BLOCK, h * wide : (h + 1) * wide].astype(jnp.float32)
            )
            mix[b * BLOCK : (b + 1) * BLOCK, h * wide : (h + 1) * wide] = (
                gate * cell * norm * head_scale_ref[:, h * wide : (h + 1) * wide]
            ).astype(jnp.bfloat16)
        for target in range(tp_size):
            if b == ((target + 1) * share - 1) // BLOCK:
                @pl.when(tp != target)
                def _(target=target):
                    mix_copy(tp, target).start()

    token_mix[:, pl.ds(pl.multiple_of(tp * columns, columns), columns)] = mix[
        pl.ds(pl.multiple_of(tp * share, share), share), :
    ]
    weight_copy.wait()
    for k in range(1, tp_size):
        mix_copy(lax.rem(tp + k, tp_size), tp).wait_recv()
    width = weights.shape[1]
    tile = 512

    def project(t, squares):
        where = pl.ds(pl.multiple_of(t * tile, tile), tile)
        middle = (
            residual_ref[:, where].astype(jnp.float32)
            + dot_f32(token_mix[...], weights[:, where])
        ).astype(jnp.bfloat16)
        middle = middle.astype(jnp.float32)
        outcome[:, where] = middle
        return squares + jnp.sum(middle * middle, axis=-1, keepdims=True)

    squares = lax.fori_loop(
        0, width // tile, project, jnp.zeros((share, 1), jnp.float32)
    )
    norm = lax.rsqrt(squares * (1.0 / width) + epsilon)

    publish(norm, norm_scale_ref)

    def finish(k, carry):
        @pl.when(sp + k < n)
        def _():
            for copy in state_copies(sp, sp + k):
                copy.wait_send()

        return carry

    lax.fori_loop(1, n, finish, 0)
    for k in range(1, tp_size):
        mix_copy(tp, lax.rem(tp + k, tp_size)).wait_send()


def greet_sp(n):
    sp = lax.axis_index("sp")
    barrier = pltpu.get_barrier_semaphore()

    def one(k, carry):
        pl.semaphore_signal(
            barrier, inc=1, device_id={"sp": lax.rem(sp + k, n)}, device_id_type=MESH
        )
        return carry

    lax.fori_loop(1, n, one, 0)


def cell_kernel(n, tp_size, heads, experts, slots, *refs):
    inputs, (middle_ref, normed_ref, notes_ref), scratch = refs[:13], refs[13:16], refs[16:]
    outcome = scratch[0]
    tp = lax.axis_index("tp")
    greet_sp(n)
    for k in range(1, tp_size):
        pl.semaphore_signal(
            pltpu.get_barrier_semaphore(), inc=1,
            device_id={"tp": lax.rem(tp + k, tp_size)}, device_id_type=MESH,
        )

    def publish(norm, norm_scale_ref):
        middle_ref[...] = outcome[...].astype(jnp.bfloat16)
        normed_ref[...] = (outcome[...] * norm * norm_scale_ref[...]).astype(jnp.bfloat16)

    cell_body(n, tp_size, heads, experts, slots, inputs, (notes_ref,) + scratch,
              n + tp_size - 2, lambda: None, publish)


def cell_scratch(heads, n, tp_size, queries, values, residual, projection):
    length = queries.shape[0]
    keys = queries.shape[1] // heads
    wide = values.shape[1] // heads
    rows = heads * (length // BLOCK)
    tokens, width = residual.shape
    note_rows = -(-2 * heads // 8) * 8
    dma = pltpu.SemaphoreType.DMA
    return [
        pltpu.VMEM((tokens, width), jnp.float32),
        pltpu.VMEM((heads * keys, wide), jnp.bfloat16),
        pltpu.VMEM((note_rows, wide), jnp.float32),
        pltpu.VMEM((n, heads * keys, wide), jnp.bfloat16),
        pltpu.VMEM((n, note_rows, wide), jnp.float32),
        pltpu.VMEM((rows, keys, wide), jnp.float32),
        pltpu.VMEM((rows, BLOCK, wide), jnp.float32),
        pltpu.VMEM((length, heads * wide), jnp.bfloat16),
        pltpu.VMEM((tokens, projection.shape[0]), jnp.bfloat16),
        pltpu.VMEM(projection.shape, jnp.bfloat16),
        dma((n,)), dma((n,)), dma((n,)), dma((n,)),
        dma((tp_size,)), dma((tp_size,)),
        dma(()),
    ]


def cell_call(heads, experts, slots, arrays):
    queries, values, residual, projection = arrays[0], arrays[2], arrays[8], arrays[9]
    n = lax.axis_size("sp")
    tp_size = lax.axis_size("tp")
    tokens, width = residual.shape
    vmem = pl.BlockSpec(memory_space=pltpu.VMEM)
    anywhere = pl.BlockSpec(memory_space=pl.ANY)
    specs = [vmem] * len(arrays)
    specs[9] = anywhere
    return pl.pallas_call(
        functools.partial(cell_kernel, n, tp_size, heads, experts, slots),
        out_shape=(
            jax.ShapeDtypeStruct((tokens, width), jnp.bfloat16),
            jax.ShapeDtypeStruct((tokens, width), jnp.bfloat16),
            jax.ShapeDtypeStruct((8, tokens), jnp.float32),
        ),
        in_specs=specs,
        out_specs=(vmem, vmem, vmem),
        scratch_shapes=cell_scratch(heads, n, tp_size, queries, values, residual, projection),
        compiler_params=pltpu.CompilerParams(collective_id=0, has_side_effects=True),
    )(*arrays)


def layer_kernel(n, tp_size, heads, experts, chunks, tile, *refs):
    inputs, (gate_ref, up_ref, down_ref), out_ref = refs[:13], refs[13:16], refs[16]
    (notes, rows, sent, arrived, produced, returned, activation, gate_w, up_w, down_w,
     notes_send, notes_recv, rows_send, rows_recv, there_send, there_recv,
     back_send, back_recv, weight_sems) = refs[17:36]
    cell_refs = refs[36:]
    notes_ref, outcome = cell_refs[:2]
    sp = lax.axis_index("sp")
    tp = lax.axis_index("tp")
    lanes, part = rows.shape[2:]
    halves, members, slots, wide = sent.shape[1:]
    each = chunks // halves
    width = halves * wide
    hidden = gate_w.shape[1]
    sp_rows = members // tp_size
    plane = sp // sp_rows
    member = lax.rem(sp, sp_rows) * tp_size + tp
    last = PLANES - 1
    upper = plane >= PLANES // 2
    outward = jnp.where(upper, 1, -1)
    at_end = (plane == 0) | (plane == last)

    def place(to_plane, to_member):
        return dict(
            device_id={"sp": to_plane * sp_rows + to_member // tp_size,
                       "tp": lax.rem(to_member, tp_size)},
            device_id_type=MESH,
        )

    def beside(step):
        return lax.rem(plane + step + PLANES, PLANES)

    weight_copies = [
        pltpu.make_async_copy(source.at[0], target, weight_sems.at[k])
        for k, (source, target) in enumerate(
            ((gate_ref, gate_w), (up_ref, up_w), (down_ref, down_w))
        )
    ]
    barrier = pltpu.get_barrier_semaphore()
    greet_sp(n)
    for k in range(1, members):
        pl.semaphore_signal(barrier, inc=1, **place(plane, lax.rem(member + k, members)))

    def notes_copy(source, target):
        return pltpu.make_async_remote_copy(
            src_ref=notes_ref, dst_ref=notes.at[source],
            send_sem=notes_send.at[target], recv_sem=notes_recv.at[source],
            **place(target, member))

    def rows_copy(block, k, step):
        return pltpu.make_async_remote_copy(
            src_ref=rows.at[block, k], dst_ref=rows.at[block, k],
            send_sem=rows_send.at[(step + 1) // 2, block, k], recv_sem=rows_recv.at[block, k],
            **place(beside(step), member))

    def there(block, half, target):
        return pltpu.make_async_remote_copy(
            src_ref=sent.at[block, half, target], dst_ref=arrived.at[block, half, member],
            send_sem=there_send.at[block, half], recv_sem=there_recv.at[block, half],
            **place(plane, target))

    def back(block, half, target):
        return pltpu.make_async_remote_copy(
            src_ref=produced.at[block, half, target],
            dst_ref=returned.at[plane, half, member],
            send_sem=back_send.at[block, half], recv_sem=back_recv.at[plane, half],
            **place(block, target))

    def bytes_of(buffer, block, half, sem, count):
        span = buffer.at[block, half, pl.ds(0, count)]
        return pltpu.make_async_copy(span, span, sem.at[block, half])

    def announce():
        for k in range(1, PLANES):
            notes_copy(plane, beside(k)).start()
        notes[plane] = notes_ref[...]
        for copy in weight_copies:
            copy.start()

    def send_rows(k):
        for step in (1, -1):
            @pl.when((plane + step >= 0) & (plane + step <= last))
            def _(step=step):
                rows_copy(plane, k, step).start()

    def publish(norm, norm_scale_ref):
        for k in range(chunks):
            columns = slice(k * part, (k + 1) * part)
            rows[plane, k] = (outcome[:, columns] * norm * norm_scale_ref[:, columns]).astype(
                jnp.bfloat16
            )
            if k > 0:
                send_rows(k - 1)
        send_rows(chunks - 1)

    cell_body(n, tp_size, heads, experts, slots, inputs, cell_refs,
              n + members - 2, announce, publish)

    def matches(block, of_plane):
        slot = lax.broadcasted_iota(jnp.int32, (members * slots, lanes), 0)
        slot = (slot + of_plane * (members * slots)).astype(jnp.float32)
        return notes[block, 0:1, :] == slot, notes[block, 1:2, :] == slot

    def dispatch(block, half):
        first, second = matches(block, plane)
        pick = jnp.where(first | second, 1.0, 0.0).astype(jnp.bfloat16)
        for k in range(each):
            chosen = dot_f32(pick, rows[block, half * each + k]).astype(jnp.bfloat16)
            sent[block, half, :, :, k * part : (k + 1) * part] = chosen.reshape(
                members, slots, part
            )
        for i in range(1, members):
            there(block, half, lax.rem(member + i, members)).start()
        arrived[block, half, member] = sent[block, half, member]

    def take(block, half, forward):
        for k in range(half * each, (half + 1) * each):
            rows_copy(block, k, -1).wait_recv()
            if forward is not None:
                rows_copy(block, k, forward).start()
        dispatch(block, half)

    def give_back(block, half):
        for i in range(1, members):
            back(block, half, lax.rem(member + i, members)).start()
        back(block, half, member).start()

    def give_home():
        for half in range(halves):
            for i in range(1, members):
                back(plane, half, lax.rem(member + i, members)).start()
            returned[plane, half, member] = produced[plane, half, member]

    def give_late(block):
        for half in range(halves):
            give_back(block, half)

    def compute(block, send=True):
        for half in range(halves):
            bytes_of(arrived, block, half, there_recv, members - 1).wait()

        def hidden_tile(t, carry):
            columns = pl.ds(pl.multiple_of(t * tile, tile), tile)
            gate_part = up_part = 0.0
            for half in range(halves):
                tokens = arrived[block, half].reshape(members * slots, wide)
                span = slice(half * wide, (half + 1) * wide)
                gate_part = gate_part + dot_f32(tokens, gate_w[span, columns])
                up_part = up_part + dot_f32(tokens, up_w[span, columns])
            activation[:, columns] = (jax.nn.silu(gate_part) * up_part).astype(jnp.bfloat16)
            return carry

        lax.fori_loop(0, hidden // tile, hidden_tile, 0)
        for half in range(halves):
            def width_tile(t, carry):
                start = pl.multiple_of(t * tile, tile)
                result = dot_f32(
                    activation[...], down_w[:, pl.ds(half * wide + start, tile)]
                ).astype(jnp.bfloat16)
                produced[block, half, :, :, pl.ds(start, tile)] = result.reshape(
                    members, slots, tile
                )
                return carry

            lax.fori_loop(0, wide // tile, width_tile, 0)
            if send:
                give_back(block, half)


    def gather(of_plane, home=False):
        first, second = matches(plane, of_plane)
        spread = jnp.where(first, notes[plane, 2:3, :], 0.0) + jnp.where(
            second, notes[plane, 3:4, :], 0.0
        )
        high, low = split(spread.T)
        for half in range(halves):
            bytes_of(returned, of_plane, half, back_recv, members - 1 if home else members).wait()
            for k in range(each):
                share = returned[of_plane, half, :, :, k * part : (k + 1) * part].reshape(
                    members * slots, part
                )
                columns = slice(half * wide + k * part, half * wide + (k + 1) * part)
                outcome[:, columns] += dot_f32(high, share) + dot_f32(low, share)

    for half in range(halves):
        dispatch(plane, half)
    for k in range(1, PLANES):
        notes_copy(beside(k), plane).wait_recv()

    @pl.when(at_end)
    def _():
        one, two, three = plane - outward, plane - 2 * outward, plane - 3 * outward
        take(one, 0, None)
        take(one, 1, None)
        for copy in weight_copies:
            copy.wait()
        compute(plane, False)
        compute(one)
        take(two, 0, None)
        take(two, 1, None)
        give_home()
        compute(two)
        take(three, 0, None)
        take(three, 1, None)
        compute(three)
        gather(plane, True)
        gather(one)
        gather(two)
        gather(three)

    @pl.when(jnp.logical_not(at_end))
    def _():
        inner, outer, far = plane - outward, plane + outward, plane - 2 * outward
        take(inner, 0, outward)
        take(outer, 0, -outward)
        take(inner, 1, outward)
        take(outer, 1, -outward)
        for copy in weight_copies:
            copy.wait()
        compute(plane, False)
        compute(inner)
        take(far, 0, outward)
        take(far, 1, outward)
        compute(outer)
        compute(far)
        give_home()
        gather(plane, True)
        gather(outer)
        gather(inner)
        gather(far)

    out_ref[...] = outcome[...].astype(jnp.bfloat16)
    for k in range(1, PLANES):
        notes_copy(plane, beside(k)).wait_send()

    def finish(block, carry):
        @pl.when((block <= plane) & (plane < last))
        def _():
            for k in range(chunks):
                rows_copy(block, k, 1).wait_send()

        @pl.when((block >= plane) & (plane > 0))
        def _():
            for k in range(chunks):
                rows_copy(block, k, -1).wait_send()

        for half in range(halves):
            bytes_of(sent, block, half, there_send, members - 1).wait()
            bytes_of(produced, block, half, back_send, members - 1).wait()

        @pl.when(block != plane)
        def _():
            for half in range(halves):
                bytes_of(produced, block, half, back_send, 1).wait()

        return carry

    lax.fori_loop(0, PLANES, finish, 0)


def layer_call(heads, experts, slots, arrays, gate, up, down):
    queries, values, residual, projection = arrays[0], arrays[2], arrays[8], arrays[9]
    tokens, width = residual.shape
    hidden = gate.shape[2]
    n = lax.axis_size("sp")
    tp_size = lax.axis_size("tp")
    members = n * tp_size // PLANES
    chunks, halves = 4, 2
    vmem = pl.BlockSpec(memory_space=pltpu.VMEM)
    anywhere = pl.BlockSpec(memory_space=pl.ANY)
    slotted = pltpu.VMEM((PLANES, halves, members, slots, width // halves), jnp.bfloat16)
    dma = pltpu.SemaphoreType.DMA
    specs = [vmem] * len(arrays) + [anywhere] * 3
    specs[9] = anywhere
    return pl.pallas_call(
        functools.partial(layer_kernel, n, tp_size, heads, experts, chunks, 256),
        out_shape=jax.ShapeDtypeStruct(residual.shape, jnp.bfloat16),
        in_specs=specs,
        out_specs=vmem,
        scratch_shapes=[
            pltpu.VMEM((PLANES, 8, tokens), jnp.float32),
            pltpu.VMEM((PLANES, chunks, tokens, width // chunks), jnp.bfloat16),
            slotted,
            slotted,
            slotted,
            slotted,
            pltpu.VMEM((members * slots, hidden), jnp.bfloat16),
            pltpu.VMEM((width, hidden), jnp.bfloat16),
            pltpu.VMEM((width, hidden), jnp.bfloat16),
            pltpu.VMEM((hidden, width), jnp.bfloat16),
            dma((PLANES,)),
            dma((PLANES,)),
            dma((2, PLANES, chunks)),
            dma((PLANES, chunks)),
            dma((PLANES, halves)),
            dma((PLANES, halves)),
            dma((PLANES, halves)),
            dma((PLANES, halves)),
            dma((3,)),
            pltpu.VMEM((8, tokens), jnp.float32),
        ]
        + cell_scratch(heads, n, tp_size, queries, values, residual, projection),
        compiler_params=pltpu.CompilerParams(collective_id=1, has_side_effects=True),
    )(*arrays, gate, up, down)


def shards(
    queries,
    keys,
    values,
    input_gate_log,
    forget_gate_logits,
    extra_decay_log,
    output_gate_logits,
    head_norm_scale,
    layer_residual_input,
    output_projection_weight,
    expert_norm_scale,
    routing_expert_index,
    routing_expert_weight,
    expert_gate_weight,
    expert_up_weight,
    expert_down_weight,
):
    sp_count = lax.axis_size("sp")
    tp_count = lax.axis_size("tp")
    devices = sp_count * tp_count
    local_experts = expert_gate_weight.shape[0]
    experts = local_experts * devices
    tok_count, model_width = layer_residual_input.shape
    slots = max(2, 2 * tok_count * TOP // experts)
    heads = input_gate_log.shape[0]
    arrays = [
        queries, keys, values, input_gate_log, forget_gate_logits, extra_decay_log,
        output_gate_logits, head_norm_scale[None], layer_residual_input,
        output_projection_weight, expert_norm_scale[None], routing_expert_index.T,
        routing_expert_weight.T,
    ]
    if (
        local_experts == 1
        and slots % 16 == 0
        and sp_count % PLANES == 0
        and model_width % 1024 == 0
    ):
        return layer_call(
            heads, experts, slots, arrays,
            expert_gate_weight, expert_up_weight, expert_down_weight,
        )
    middle, normed, notes = cell_call(heads, experts, slots, arrays)
    slot_key = notes[:TOP].T.astype(jnp.int32).reshape(-1)
    matches = slot_key[None, :] == jnp.arange(experts * slots, dtype=jnp.int32)[:, None]
    pick = jnp.sum(
        matches.reshape(experts * slots, tok_count, TOP).astype(jnp.float32), axis=2
    ).astype(jnp.bfloat16)
    outgoing = (
        jnp.dot(pick, normed, preferred_element_type=jnp.float32)
        .astype(jnp.bfloat16)
        .reshape(experts, slots, model_width)
    )
    weight_high = lax.reduce_precision(routing_expert_weight, 8, 7)
    slot_pairs = slot_key.reshape(tok_count, TOP, 1)
    slot_range = jnp.arange(experts * slots, dtype=jnp.int32)

    def spread(weights):
        return jnp.sum(
            jnp.where(slot_pairs == slot_range, weights[:, :, None], 0.0), axis=1
        ).astype(jnp.bfloat16)

    high = spread(weight_high)
    low = spread(routing_expert_weight - weight_high)
    arrived = lax.all_to_all(outgoing, ("sp", "tp"), split_axis=0, concat_axis=0, tiled=True)
    grouped = arrived.reshape(devices, local_experts, arrived.shape[1], model_width)
    gate_part = jnp.einsum(
        "sxcd,xdf->sxcf", grouped, expert_gate_weight, preferred_element_type=jnp.float32
    )
    up_part = jnp.einsum(
        "sxcd,xdf->sxcf", grouped, expert_up_weight, preferred_element_type=jnp.float32
    )
    activation = (jax.nn.silu(gate_part) * up_part).astype(jnp.bfloat16)
    produced = jnp.einsum(
        "sxcf,xfd->sxcd", activation, expert_down_weight, preferred_element_type=jnp.float32
    ).astype(jnp.bfloat16)
    returned = lax.all_to_all(
        produced.reshape(arrived.shape), ("sp", "tp"), split_axis=0, concat_axis=0, tiled=True
    )
    returned = returned.reshape(experts * slots, model_width)
    expert_sum = jnp.dot(high, returned, preferred_element_type=jnp.float32) + jnp.dot(
        low, returned, preferred_element_type=jnp.float32
    )
    return (middle.astype(jnp.float32) + expert_sum).astype(jnp.bfloat16)


def solution(mesh):
    in_specs = (
        P("sp", "tp"),
        P("sp", "tp"),
        P("sp", "tp"),
        P("tp", "sp"),
        P("tp", "sp"),
        P("tp", "sp"),
        P("sp", "tp"),
        P("tp"),
        P(("sp", "tp"), None),
        P(),
        P(),
        P(("sp", "tp"), None),
        P(("sp", "tp"), None),
        P(("sp", "tp"), None, None),
        P(("sp", "tp"), None, None),
        P(("sp", "tp"), None, None),
    )
    out_specs = P(("sp", "tp"), None)
    return jax.shard_map(shards, mesh=mesh, in_specs=in_specs, out_specs=out_specs, check_vma=False)
```

```python
import functools

import jax
import jax.numpy as jnp
from jax import lax
from jax.experimental import pallas as pl
from jax.experimental.pallas import tpu as pltpu
from jax.sharding import PartitionSpec as P

TOP = 2
BLOCK = 128
PLANES = 4


very_low = -1e30
epsilon = 1e-06
MESH = pl.DeviceIdType.MESH


def split(value):
    high = value.astype(jnp.bfloat16)
    return high, (value - high.astype(jnp.float32)).astype(jnp.bfloat16)


def dot_f32(a, b):
    return jnp.dot(a, b, preferred_element_type=jnp.float32)


def along_lanes(value, join, empty):
    lane = lax.broadcasted_iota(jnp.int32, value.shape, 1)
    shift = 1
    while shift < value.shape[1]:
        moved = jnp.where(lane >= shift, pltpu.roll(value, shift, 1), empty)
        value = join(value, moved)
        shift *= 2
    return value


def route_notes(index_ref, weight_ref, experts, slots):
    tokens = index_ref.shape[1]
    expert = lax.broadcasted_iota(jnp.int32, (experts, tokens), 0)
    before = lax.broadcasted_iota(jnp.int32, (tokens, tokens), 0) < lax.broadcasted_iota(
        jnp.int32, (tokens, tokens), 1
    )
    before = jnp.where(before, 1.0, 0.0).astype(jnp.bfloat16)
    base = jnp.zeros((experts, 1), jnp.float32)
    lines = []
    for j in range(TOP):
        row = index_ref[j : j + 1, :]
        named = jnp.where(expert == row, 1.0, 0.0)
        seen = dot_f32(named.astype(jnp.bfloat16), before) + base
        position = jnp.sum(named * seen, axis=0, keepdims=True)
        lines.append(row.astype(jnp.float32) * slots + position)
        base = base + jnp.sum(named, axis=1, keepdims=True)
    lines += [weight_ref[j : j + 1, :] for j in range(TOP)]
    lines.append(jnp.zeros((8 - 2 * TOP, tokens), jnp.float32))
    return jnp.concatenate(lines, axis=0)


def cell_body(n, tp_size, heads, experts, slots, inputs, scratch, barrier_count, announce, settled, mixed, publish):
    (query_ref, key_ref, value_ref, input_ref, forget_ref, extra_ref, gate_ref, head_scale_ref,
     residual_ref, projection_ref, norm_scale_ref, index_ref, weight_ref) = inputs
    (notes_ref, outcome, state, state_notes, got_state, got_notes, carried, intra, mix, token_mix,
     weights, send_state, send_notes, recv_state, recv_notes, send_mix, recv_mix,
     weight_sem) = scratch
    sp = lax.axis_index("sp")
    tp = lax.axis_index("tp")
    length = query_ref.shape[0]
    blocks = length // BLOCK
    keys = query_ref.shape[1] // heads
    wide = value_ref.shape[1] // heads
    share = length // tp_size
    columns = heads * wide

    weight_copy = pltpu.make_async_copy(projection_ref, weights, weight_sem)
    weight_copy.start()
    barrier = pltpu.get_barrier_semaphore()

    def state_copies(source, target):
        kind = dict(device_id={"sp": target}, device_id_type=MESH)
        return (
            pltpu.make_async_remote_copy(
                src_ref=state, dst_ref=got_state.at[source],
                send_sem=send_state.at[target], recv_sem=recv_state.at[source], **kind),
            pltpu.make_async_remote_copy(
                src_ref=state_notes, dst_ref=got_notes.at[source],
                send_sem=send_notes.at[target], recv_sem=recv_notes.at[source], **kind),
        )

    def mix_copy(source, target):
        return pltpu.make_async_remote_copy(
            src_ref=mix.at[pl.ds(target * share, share), :],
            dst_ref=token_mix.at[:, pl.ds(pl.multiple_of(source * columns, columns), columns)],
            send_sem=send_mix.at[target], recv_sem=recv_mix.at[source],
            device_id={"tp": target}, device_id_type=MESH)

    def by_block(value):
        return jnp.concatenate(
            [value[h : h + 1, b * BLOCK : (b + 1) * BLOCK]
             for h in range(heads) for b in range(blocks)], axis=0)

    logits = forget_ref[...]
    decay = jnp.minimum(logits, 0.0) - jnp.log1p(jnp.exp(-jnp.abs(logits))) + extra_ref[...]
    within = along_lanes(by_block(decay), jnp.add, 0.0)
    level = by_block(input_ref[...]) - within
    peak = along_lanes(level, jnp.maximum, very_low)
    total = within[:, BLOCK - 1 : BLOCK]
    top = peak[:, BLOCK - 1 : BLOCK]
    state_add = jnp.exp(level - top)
    block_max = total + top
    largest = within + peak

    keys_t = key_ref[...].astype(jnp.float32).T
    keys_t_low = keys_t.astype(jnp.bfloat16)
    zero = jnp.zeros((1, 1), jnp.float32)
    state_notes[...] = jnp.zeros_like(state_notes)
    local_max, local_before = [], []
    for h in range(heads):
        memory = jnp.zeros((keys, wide), jnp.float32)
        high_mark = jnp.full((1, 1), very_low, jnp.float32)
        passed = zero
        for b in range(blocks):
            row = h * blocks + b
            carried[row] = memory
            local_max.append(high_mark)
            local_before.append(passed)
            added_high, added_low = split(
                keys_t[h * keys : (h + 1) * keys, b * BLOCK : (b + 1) * BLOCK]
                * state_add[row : row + 1, :]
            )
            values = value_ref[b * BLOCK : (b + 1) * BLOCK, h * wide : (h + 1) * wide]
            added = dot_f32(added_high, values) + dot_f32(added_low, values)
            shifted = high_mark + total[row : row + 1]
            combined = jnp.maximum(shifted, block_max[row : row + 1])
            memory = jnp.exp(shifted - combined) * memory + jnp.exp(
                block_max[row : row + 1] - combined
            ) * added
            high_mark = combined
            passed = passed + total[row : row + 1]
        state[h * keys : (h + 1) * keys, :] = memory.astype(jnp.bfloat16)
        state_notes[h : h + 1, :] = jnp.broadcast_to(passed, (1, wide))
        state_notes[heads + h : heads + h + 1, :] = jnp.broadcast_to(high_mark, (1, wide))
    pl.semaphore_wait(barrier, barrier_count)

    def send_on(k, carry):
        @pl.when(sp + n - k < n)
        def _():
            for copy in state_copies(sp, sp + n - k):
                copy.start()

        return carry

    lax.fori_loop(1, n, send_on, 0)

    notes_ref[...] = route_notes(index_ref, weight_ref, experts, slots)
    announce()
    causal = lax.broadcasted_iota(jnp.int32, (BLOCK, BLOCK), 0) >= lax.broadcasted_iota(
        jnp.int32, (BLOCK, BLOCK), 1
    )
    lane = lax.broadcasted_iota(jnp.int32, (BLOCK, heads * keys), 1)
    peak_t = peak.T

    def own_query(h, b):
        query = query_ref[b * BLOCK : (b + 1) * BLOCK, :] * jnp.bfloat16(keys ** -0.5)
        return jnp.where(
            (lane >= h * keys) & (lane < (h + 1) * keys), query, jnp.zeros_like(query)
        )

    for h in range(heads):
        for b in range(blocks):
            row = h * blocks + b
            scores = dot_f32(own_query(h, b), keys_t_low[:, b * BLOCK : (b + 1) * BLOCK])
            weight = jnp.exp(
                jnp.where(causal, level[row : row + 1, :] - peak_t[:, row : row + 1], very_low)
            )
            score_high, score_low = split(scores * weight)
            values = value_ref[b * BLOCK : (b + 1) * BLOCK, h * wide : (h + 1) * wide]
            intra[row] = dot_f32(score_high, values) + dot_f32(score_low, values)

    def lap(j, carry):
        memory, marks = carry
        for copy in state_copies(j, sp):
            copy.wait_recv()
        memories, later = [], []
        for h in range(heads):
            passed = got_notes[j, h : h + 1, :]
            late = got_notes[j, heads + h : heads + h + 1, :]
            shifted = passed + marks[h : h + 1, :]
            combined = jnp.maximum(shifted, late)
            memories.append(
                jnp.exp(shifted - combined) * memory[h * keys : (h + 1) * keys, :]
                + jnp.exp(late - combined)
                * got_state[j, h * keys : (h + 1) * keys, :].astype(jnp.float32)
            )
            later.append(combined)
        return jnp.concatenate(memories, axis=0), jnp.concatenate(later, axis=0)

    earlier, marks = lax.fori_loop(
        0, sp, lap,
        (jnp.zeros((heads * keys, wide), jnp.float32), jnp.zeros((heads, wide), jnp.float32)),
    )

    settled()
    local_marks = jnp.concatenate(local_max, axis=0)
    moved_marks = jnp.concatenate(local_before, axis=0) + jnp.concatenate(
        [marks[h : h + 1, 0:1] for h in range(heads) for _ in range(blocks)], axis=0
    )
    start_marks = jnp.maximum(moved_marks, local_marks)
    moved_scale = jnp.exp(moved_marks - start_marks)
    local_scale = jnp.exp(local_marks - start_marks)
    from_start = within + start_marks
    joined = jnp.maximum(largest, from_start)
    scales = jnp.concatenate(
        [jnp.exp(largest - joined), jnp.exp(from_start - joined)], axis=0
    ).T
    rows = heads * blocks

    for b in range(blocks):
        for h in range(heads):
            row = h * blocks + b
            start = (
                moved_scale[row : row + 1] * earlier[h * keys : (h + 1) * keys, :]
                + local_scale[row : row + 1] * carried[row]
            )
            start_high, start_low = split(start)
            query = query_ref[b * BLOCK : (b + 1) * BLOCK, h * keys : (h + 1) * keys]
            query = query * jnp.bfloat16(keys ** -0.5)
            cell = scales[:, row : row + 1] * intra[row] + scales[
                :, rows + row : rows + row + 1
            ] * (dot_f32(query, start_high) + dot_f32(query, start_low))
            norm = lax.rsqrt(jnp.mean(cell * cell, axis=-1, keepdims=True) + epsilon)
            gate = jax.nn.sigmoid(
                gate_ref[b * BLOCK : (b + 1) * BLOCK, h * wide : (h + 1) * wide].astype(jnp.float32)
            )
            mix[b * BLOCK : (b + 1) * BLOCK, h * wide : (h + 1) * wide] = (
                gate * cell * norm * head_scale_ref[:, h * wide : (h + 1) * wide]
            ).astype(jnp.bfloat16)
        for target in range(tp_size):
            if b == ((target + 1) * share - 1) // BLOCK:
                @pl.when(tp != target)
                def _(target=target):
                    mix_copy(tp, target).start()

    token_mix[:, pl.ds(pl.multiple_of(tp * columns, columns), columns)] = mix[
        pl.ds(pl.multiple_of(tp * share, share), share), :
    ]
    weight_copy.wait()
    for k in range(1, tp_size):
        mix_copy(lax.rem(tp + k, tp_size), tp).wait_recv()
    mixed()
    width = weights.shape[1]
    tile = 512

    def project(t, squares):
        where = pl.ds(pl.multiple_of(t * tile, tile), tile)
        middle = (
            residual_ref[:, where].astype(jnp.float32)
            + dot_f32(token_mix[...], weights[:, where])
        ).astype(jnp.bfloat16)
        middle = middle.astype(jnp.float32)
        outcome[:, where] = middle
        return squares + jnp.sum(middle * middle, axis=-1, keepdims=True)

    squares = lax.fori_loop(
        0, width // tile, project, jnp.zeros((share, 1), jnp.float32)
    )
    norm = lax.rsqrt(squares * (1.0 / width) + epsilon)

    publish(norm, norm_scale_ref)

    def finish(k, carry):
        @pl.when(sp + k < n)
        def _():
            for copy in state_copies(sp, sp + k):
                copy.wait_send()

        return carry

    lax.fori_loop(1, n, finish, 0)
    for k in range(1, tp_size):
        mix_copy(tp, lax.rem(tp + k, tp_size)).wait_send()


def greet_sp(n):
    sp = lax.axis_index("sp")
    barrier = pltpu.get_barrier_semaphore()

    def one(k, carry):
        pl.semaphore_signal(
            barrier, inc=1, device_id={"sp": lax.rem(sp + k, n)}, device_id_type=MESH
        )
        return carry

    lax.fori_loop(1, n, one, 0)


def cell_kernel(n, tp_size, heads, experts, slots, *refs):
    inputs, (middle_ref, normed_ref, notes_ref), scratch = refs[:13], refs[13:16], refs[16:]
    outcome = scratch[0]
    tp = lax.axis_index("tp")
    greet_sp(n)
    for k in range(1, tp_size):
        pl.semaphore_signal(
            pltpu.get_barrier_semaphore(), inc=1,
            device_id={"tp": lax.rem(tp + k, tp_size)}, device_id_type=MESH,
        )

    def publish(norm, norm_scale_ref):
        middle_ref[...] = outcome[...].astype(jnp.bfloat16)
        normed_ref[...] = (outcome[...] * norm * norm_scale_ref[...]).astype(jnp.bfloat16)

    cell_body(n, tp_size, heads, experts, slots, inputs, (notes_ref,) + scratch,
              n + tp_size - 2, lambda: None, lambda: None, lambda: None, publish)


def cell_scratch(heads, n, tp_size, queries, values, residual, projection):
    length = queries.shape[0]
    keys = queries.shape[1] // heads
    wide = values.shape[1] // heads
    rows = heads * (length // BLOCK)
    tokens, width = residual.shape
    note_rows = -(-2 * heads // 8) * 8
    dma = pltpu.SemaphoreType.DMA
    return [
        pltpu.VMEM((tokens, width), jnp.float32),
        pltpu.VMEM((heads * keys, wide), jnp.bfloat16),
        pltpu.VMEM((note_rows, wide), jnp.float32),
        pltpu.VMEM((n, heads * keys, wide), jnp.bfloat16),
        pltpu.VMEM((n, note_rows, wide), jnp.float32),
        pltpu.VMEM((rows, keys, wide), jnp.float32),
        pltpu.VMEM((rows, BLOCK, wide), jnp.float32),
        pltpu.VMEM((length, heads * wide), jnp.bfloat16),
        pltpu.VMEM((tokens, projection.shape[0]), jnp.bfloat16),
        pltpu.VMEM(projection.shape, jnp.bfloat16),
        dma((n,)), dma((n,)), dma((n,)), dma((n,)),
        dma((tp_size,)), dma((tp_size,)),
        dma(()),
    ]


def cell_call(heads, experts, slots, arrays):
    queries, values, residual, projection = arrays[0], arrays[2], arrays[8], arrays[9]
    n = lax.axis_size("sp")
    tp_size = lax.axis_size("tp")
    tokens, width = residual.shape
    vmem = pl.BlockSpec(memory_space=pltpu.VMEM)
    anywhere = pl.BlockSpec(memory_space=pl.ANY)
    specs = [vmem] * len(arrays)
    specs[9] = anywhere
    return pl.pallas_call(
        functools.partial(cell_kernel, n, tp_size, heads, experts, slots),
        out_shape=(
            jax.ShapeDtypeStruct((tokens, width), jnp.bfloat16),
            jax.ShapeDtypeStruct((tokens, width), jnp.bfloat16),
            jax.ShapeDtypeStruct((8, tokens), jnp.float32),
        ),
        in_specs=specs,
        out_specs=(vmem, vmem, vmem),
        scratch_shapes=cell_scratch(heads, n, tp_size, queries, values, residual, projection),
        compiler_params=pltpu.CompilerParams(collective_id=0, has_side_effects=True),
    )(*arrays)


def layer_kernel(n, tp_size, heads, experts, chunks, tile, *refs):
    inputs, (gate_ref, up_ref, down_ref), out_ref = refs[:13], refs[13:16], refs[16]
    (notes, rows, sent, arrived, produced, returned, activation, gate_w, up_w, down_w,
     notes_send, notes_recv, rows_send, rows_recv, there_send, there_recv,
     back_send, back_recv, weight_sems, residual_in, mix_in, residual_send, residual_recv,
     mix_send, mix_recv) = refs[17:42]
    cell_refs = refs[42:]
    notes_ref, outcome = cell_refs[:2]
    token_mix, projection = cell_refs[9:11]
    residual_ref, norm_scale = inputs[8], inputs[10]
    sp = lax.axis_index("sp")
    tp = lax.axis_index("tp")
    lanes, part = rows.shape[2:]
    halves, members, slots, wide = sent.shape[1:]
    each = chunks // halves
    width = halves * wide
    hidden = gate_w.shape[1]
    sp_rows = members // tp_size
    plane = sp // sp_rows
    member = lax.rem(sp, sp_rows) * tp_size + tp
    last = PLANES - 1
    upper = plane >= PLANES // 2
    outward = jnp.where(upper, 1, -1)
    at_end = (plane == 0) | (plane == last)

    def place(to_plane, to_member):
        return dict(
            device_id={"sp": to_plane * sp_rows + to_member // tp_size,
                       "tp": lax.rem(to_member, tp_size)},
            device_id_type=MESH,
        )

    def beside(step):
        return lax.rem(plane + step + PLANES, PLANES)

    weight_copies = [
        pltpu.make_async_copy(source.at[0], target, weight_sems.at[k])
        for k, (source, target) in enumerate(
            ((gate_ref, gate_w), (up_ref, up_w), (down_ref, down_w))
        )
    ]
    barrier = pltpu.get_barrier_semaphore()
    greet_sp(n)
    for k in range(1, members):
        pl.semaphore_signal(barrier, inc=1, **place(plane, lax.rem(member + k, members)))

    def notes_copy(source, target):
        return pltpu.make_async_remote_copy(
            src_ref=notes_ref, dst_ref=notes.at[source],
            send_sem=notes_send.at[target], recv_sem=notes_recv.at[source],
            **place(target, member))

    def rows_copy(block, k, step):
        return pltpu.make_async_remote_copy(
            src_ref=rows.at[block, k], dst_ref=rows.at[block, k],
            send_sem=rows_send.at[(step + 1) // 2, block, k], recv_sem=rows_recv.at[block, k],
            **place(beside(step), member))

    def residual_copy(k, step):
        side = (1 - step) // 2
        return pltpu.make_async_remote_copy(
            src_ref=residual_ref.at[:, pl.ds(k * part, part)], dst_ref=residual_in.at[side, k],
            send_sem=residual_send.at[side, k], recv_sem=residual_recv.at[side, k],
            **place(beside(step), member))

    def mix_copy(step):
        side = (1 - step) // 2
        return pltpu.make_async_remote_copy(
            src_ref=token_mix, dst_ref=mix_in.at[side],
            send_sem=mix_send.at[side], recv_sem=mix_recv.at[side],
            **place(beside(step), member))

    def to_neighbours(run):
        for step in (1, -1):
            pl.when((plane + step >= 0) & (plane + step <= last))(functools.partial(run, step))

    def there(block, half, target):
        return pltpu.make_async_remote_copy(
            src_ref=sent.at[block, half, target], dst_ref=arrived.at[block, half, member],
            send_sem=there_send.at[block, half], recv_sem=there_recv.at[block, half],
            **place(plane, target))

    def back(block, half, target):
        return pltpu.make_async_remote_copy(
            src_ref=produced.at[block, half, target],
            dst_ref=returned.at[plane, half, member],
            send_sem=back_send.at[block, half], recv_sem=back_recv.at[plane, half],
            **place(block, target))

    def bytes_of(buffer, block, half, sem, count):
        span = buffer.at[block, half, pl.ds(0, count)]
        return pltpu.make_async_copy(span, span, sem.at[block, half])

    def announce():
        for k in range(1, PLANES):
            notes_copy(plane, beside(k)).start()

        notes[plane] = notes_ref[...]
        for copy in weight_copies:
            copy.start()

    def settled():
        def send_residual(step):
            for k in range(chunks):
                residual_copy(k, step).start()

        to_neighbours(send_residual)

    def mixed():
        to_neighbours(lambda step: mix_copy(step).start())

    def publish(norm, norm_scale_ref):
        for k in range(chunks):
            columns = slice(k * part, (k + 1) * part)
            rows[plane, k] = (outcome[:, columns] * norm * norm_scale_ref[:, columns]).astype(
                jnp.bfloat16
            )

    cell_body(n, tp_size, heads, experts, slots, inputs, cell_refs,
              n + members - 2, announce, settled, mixed, publish)

    def matches(block, of_plane):
        slot = lax.broadcasted_iota(jnp.int32, (members * slots, lanes), 0)
        slot = (slot + of_plane * (members * slots)).astype(jnp.float32)
        return notes[block, 0:1, :] == slot, notes[block, 1:2, :] == slot

    def dispatch(block, half):
        first, second = matches(block, plane)
        pick = jnp.where(first | second, 1.0, 0.0).astype(jnp.bfloat16)
        for k in range(each):
            chosen = dot_f32(pick, rows[block, half * each + k]).astype(jnp.bfloat16)
            sent[block, half, :, :, k * part : (k + 1) * part] = chosen.reshape(
                members, slots, part
            )
        for i in range(1, members):
            there(block, half, lax.rem(member + i, members)).start()
        arrived[block, half, member] = sent[block, half, member]

    def rebuild(block, side, forward):
        mix_copy(1 - 2 * side).wait_recv()
        squares = jnp.zeros((lanes, 1), jnp.float32)
        for k in range(chunks):
            residual_copy(k, 1 - 2 * side).wait_recv()
            columns = slice(k * part, (k + 1) * part)
            middle = (
                residual_in[side, k].astype(jnp.float32)
                + dot_f32(mix_in[side], projection[:, columns])
            ).astype(jnp.bfloat16)
            rows[block, k] = middle
            middle = middle.astype(jnp.float32)
            squares = squares + jnp.sum(middle * middle, axis=-1, keepdims=True)
        norm = lax.rsqrt(squares * (1.0 / width) + epsilon)
        for k in range(chunks):
            columns = slice(k * part, (k + 1) * part)
            rows[block, k] = (
                rows[block, k].astype(jnp.float32) * norm * norm_scale[:, columns]
            ).astype(jnp.bfloat16)
        for half in range(halves):
            dispatch(block, half)
            if forward is not None:
                for k in range(half * each, (half + 1) * each):
                    rows_copy(block, k, forward).start()

    def take(block, half, forward):
        for k in range(half * each, (half + 1) * each):
            rows_copy(block, k, -1).wait_recv()
            if forward is not None:
                rows_copy(block, k, forward).start()
        dispatch(block, half)

    def give_back(block, half):
        back(block, half, member).start()
        for i in range(1, members):
            back(block, half, lax.rem(member + i, members)).start()

    def give_home():
        for half in range(halves):
            for i in range(1, members):
                back(plane, half, lax.rem(member + i, members)).start()
            returned[plane, half, member] = produced[plane, half, member]

    def give_late(block):
        for half in range(halves):
            give_back(block, half)

    def compute(block, send=True):
        for half in range(halves):
            bytes_of(arrived, block, half, there_recv, members - 1).wait()

        def hidden_tile(t, carry):
            columns = pl.ds(pl.multiple_of(t * tile, tile), tile)
            gate_part = up_part = 0.0
            for half in range(halves):
                tokens = arrived[block, half].reshape(members * slots, wide)
                span = slice(half * wide, (half + 1) * wide)
                gate_part = gate_part + dot_f32(tokens, gate_w[span, columns])
                up_part = up_part + dot_f32(tokens, up_w[span, columns])
            activation[:, columns] = (jax.nn.silu(gate_part) * up_part).astype(jnp.bfloat16)
            return carry

        lax.fori_loop(0, hidden // tile, hidden_tile, 0)
        for half in range(halves):
            def width_tile(t, carry):
                start = pl.multiple_of(t * tile, tile)
                result = dot_f32(
                    activation[...], down_w[:, pl.ds(half * wide + start, tile)]
                ).astype(jnp.bfloat16)
                produced[block, half, :, :, pl.ds(start, tile)] = result.reshape(
                    members, slots, tile
                )
                return carry

            lax.fori_loop(0, wide // tile, width_tile, 0)
            if send:
                give_back(block, half)


    def gather(of_plane, home=False):
        first, second = matches(plane, of_plane)
        spread = jnp.where(first, notes[plane, 2:3, :], 0.0) + jnp.where(
            second, notes[plane, 3:4, :], 0.0
        )
        high, low = split(spread.T)
        for half in range(halves):
            bytes_of(returned, of_plane, half, back_recv, members - 1 if home else members).wait()
            for k in range(each):
                share = returned[of_plane, half, :, :, k * part : (k + 1) * part].reshape(
                    members * slots, part
                )
                columns = slice(half * wide + k * part, half * wide + (k + 1) * part)
                outcome[:, columns] += dot_f32(high, share) + dot_f32(low, share)

    for half in range(halves):
        dispatch(plane, half)
    for k in range(1, PLANES):
        notes_copy(beside(k), plane).wait_recv()

    @pl.when(at_end)
    def _():
        one, two, three = plane - outward, plane - 2 * outward, plane - 3 * outward
        rebuild(one, jnp.where(upper, 0, 1), None)
        for copy in weight_copies:
            copy.wait()
        compute(plane, False)
        compute(one)
        take(two, 0, None)
        take(two, 1, None)
        give_home()
        compute(two)
        take(three, 0, None)
        take(three, 1, None)
        compute(three)
        gather(plane, True)
        gather(one)
        gather(two)
        gather(three)

    @pl.when(jnp.logical_not(at_end))
    def _():
        inner, outer, far = plane - outward, plane + outward, plane - 2 * outward
        rebuild(inner, jnp.where(upper, 0, 1), outward)
        rebuild(outer, jnp.where(upper, 1, 0), -outward)
        for copy in weight_copies:
            copy.wait()
        compute(plane, False)
        compute(inner, False)
        take(far, 0, outward)
        take(far, 1, outward)
        give_late(inner)
        compute(outer)
        compute(far)
        give_home()
        gather(plane, True)
        gather(outer)
        gather(inner)
        gather(far)

    out_ref[...] = outcome[...].astype(jnp.bfloat16)
    for k in range(1, PLANES):
        notes_copy(plane, beside(k)).wait_send()

    def sent_early(step):
        mix_copy(step).wait_send()
        for k in range(chunks):
            residual_copy(k, step).wait_send()

    to_neighbours(sent_early)

    def finish(block, carry):
        @pl.when((block < plane) & (plane < last))
        def _():
            for k in range(chunks):
                rows_copy(block, k, 1).wait_send()

        @pl.when((block > plane) & (plane > 0))
        def _():
            for k in range(chunks):
                rows_copy(block, k, -1).wait_send()

        for half in range(halves):
            bytes_of(sent, block, half, there_send, members - 1).wait()
            bytes_of(produced, block, half, back_send, members - 1).wait()

        @pl.when(block != plane)
        def _():
            for half in range(halves):
                bytes_of(produced, block, half, back_send, 1).wait()

        return carry

    lax.fori_loop(0, PLANES, finish, 0)


def layer_call(heads, experts, slots, arrays, gate, up, down):
    queries, values, residual, projection = arrays[0], arrays[2], arrays[8], arrays[9]
    tokens, width = residual.shape
    hidden = gate.shape[2]
    n = lax.axis_size("sp")
    tp_size = lax.axis_size("tp")
    members = n * tp_size // PLANES
    chunks, halves = 4, 2
    vmem = pl.BlockSpec(memory_space=pltpu.VMEM)
    anywhere = pl.BlockSpec(memory_space=pl.ANY)
    slotted = pltpu.VMEM((PLANES, halves, members, slots, width // halves), jnp.bfloat16)
    dma = pltpu.SemaphoreType.DMA
    specs = [vmem] * len(arrays) + [anywhere] * 3
    specs[9] = anywhere
    return pl.pallas_call(
        functools.partial(layer_kernel, n, tp_size, heads, experts, chunks, 512),
        out_shape=jax.ShapeDtypeStruct(residual.shape, jnp.bfloat16),
        in_specs=specs,
        out_specs=vmem,
        scratch_shapes=[
            pltpu.VMEM((PLANES, 8, tokens), jnp.float32),
            pltpu.VMEM((PLANES, chunks, tokens, width // chunks), jnp.bfloat16),
            slotted,
            slotted,
            slotted,
            slotted,
            pltpu.VMEM((members * slots, hidden), jnp.bfloat16),
            pltpu.VMEM((width, hidden), jnp.bfloat16),
            pltpu.VMEM((width, hidden), jnp.bfloat16),
            pltpu.VMEM((hidden, width), jnp.bfloat16),
            dma((PLANES,)),
            dma((PLANES,)),
            dma((2, PLANES, chunks)),
            dma((PLANES, chunks)),
            dma((PLANES, halves)),
            dma((PLANES, halves)),
            dma((PLANES, halves)),
            dma((PLANES, halves)),
            dma((3,)),
            pltpu.VMEM((2, chunks, tokens, width // chunks), jnp.bfloat16),
            pltpu.VMEM((2, tokens, projection.shape[0]), jnp.bfloat16),
            dma((2, chunks)),
            dma((2, chunks)),
            dma((2,)),
            dma((2,)),
            pltpu.VMEM((8, tokens), jnp.float32),
        ]
        + cell_scratch(heads, n, tp_size, queries, values, residual, projection),
        compiler_params=pltpu.CompilerParams(collective_id=1, has_side_effects=True),
    )(*arrays, gate, up, down)


def shards(
    queries,
    keys,
    values,
    input_gate_log,
    forget_gate_logits,
    extra_decay_log,
    output_gate_logits,
    head_norm_scale,
    layer_residual_input,
    output_projection_weight,
    expert_norm_scale,
    routing_expert_index,
    routing_expert_weight,
    expert_gate_weight,
    expert_up_weight,
    expert_down_weight,
):
    sp_count = lax.axis_size("sp")
    tp_count = lax.axis_size("tp")
    devices = sp_count * tp_count
    local_experts = expert_gate_weight.shape[0]
    experts = local_experts * devices
    tok_count, model_width = layer_residual_input.shape
    slots = max(2, 2 * tok_count * TOP // experts)
    heads = input_gate_log.shape[0]
    arrays = [
        queries, keys, values, input_gate_log, forget_gate_logits, extra_decay_log,
        output_gate_logits, head_norm_scale[None], layer_residual_input,
        output_projection_weight, expert_norm_scale[None], routing_expert_index.T,
        routing_expert_weight.T,
    ]
    if (
        local_experts == 1
        and slots % 16 == 0
        and sp_count % PLANES == 0
        and model_width % 1024 == 0
    ):
        return layer_call(
            heads, experts, slots, arrays,
            expert_gate_weight, expert_up_weight, expert_down_weight,
        )
    middle, normed, notes = cell_call(heads, experts, slots, arrays)
    slot_key = notes[:TOP].T.astype(jnp.int32).reshape(-1)
    matches = slot_key[None, :] == jnp.arange(experts * slots, dtype=jnp.int32)[:, None]
    pick = jnp.sum(
        matches.reshape(experts * slots, tok_count, TOP).astype(jnp.float32), axis=2
    ).astype(jnp.bfloat16)
    outgoing = (
        jnp.dot(pick, normed, preferred_element_type=jnp.float32)
        .astype(jnp.bfloat16)
        .reshape(experts, slots, model_width)
    )
    weight_high = lax.reduce_precision(routing_expert_weight, 8, 7)
    slot_pairs = slot_key.reshape(tok_count, TOP, 1)
    slot_range = jnp.arange(experts * slots, dtype=jnp.int32)

    def spread(weights):
        return jnp.sum(
            jnp.where(slot_pairs == slot_range, weights[:, :, None], 0.0), axis=1
        ).astype(jnp.bfloat16)

    high = spread(weight_high)
    low = spread(routing_expert_weight - weight_high)
    arrived = lax.all_to_all(outgoing, ("sp", "tp"), split_axis=0, concat_axis=0, tiled=True)
    grouped = arrived.reshape(devices, local_experts, arrived.shape[1], model_width)
    gate_part = jnp.einsum(
        "sxcd,xdf->sxcf", grouped, expert_gate_weight, preferred_element_type=jnp.float32
    )
    up_part = jnp.einsum(
        "sxcd,xdf->sxcf", grouped, expert_up_weight, preferred_element_type=jnp.float32
    )
    activation = (jax.nn.silu(gate_part) * up_part).astype(jnp.bfloat16)
    produced = jnp.einsum(
        "sxcf,xfd->sxcd", activation, expert_down_weight, preferred_element_type=jnp.float32
    ).astype(jnp.bfloat16)
    returned = lax.all_to_all(
        produced.reshape(arrived.shape), ("sp", "tp"), split_axis=0, concat_axis=0, tiled=True
    )
    returned = returned.reshape(experts * slots, model_width)
    expert_sum = jnp.dot(high, returned, preferred_element_type=jnp.float32) + jnp.dot(
        low, returned, preferred_element_type=jnp.float32
    )
    return (middle.astype(jnp.float32) + expert_sum).astype(jnp.bfloat16)


def solution(mesh):
    in_specs = (
        P("sp", "tp"),
        P("sp", "tp"),
        P("sp", "tp"),
        P("tp", "sp"),
        P("tp", "sp"),
        P("tp", "sp"),
        P("sp", "tp"),
        P("tp"),
        P(("sp", "tp"), None),
        P(),
        P(),
        P(("sp", "tp"), None),
        P(("sp", "tp"), None),
        P(("sp", "tp"), None, None),
        P(("sp", "tp"), None, None),
        P(("sp", "tp"), None, None),
    )
    out_specs = P(("sp", "tp"), None)
    return jax.shard_map(shards, mesh=mesh, in_specs=in_specs, out_specs=out_specs, check_vma=False)
```
